256 devices in a mesh: fs: 64 (over z, x, core), tp: 4 (over y).
Axes of the slice: x: 4, y: 4, z: 8, core: 2. Of those that a mesh axis runs over, the one named last changes fastest.
Arguments:
- inputs: bfloat16 [24576, 2048], P('fs'), may hold values from -6 to 6
- queries: bfloat16 [24576, 2048], P('fs', 'tp'), may hold values from -6 to 6
- keys: bfloat16 [24576, 2048], P('fs', 'tp'), may hold values from -6 to 6
- values: bfloat16 [24576, 2048], P('fs', 'tp'), may hold values from -6 to 6
- head_cot: bfloat16 [24576, 2048], P('fs', 'tp'), may hold values from -6 to 6
- mixing: float32 [16], P('tp'), may hold values from 0.3 to 0.8
- head_gain: float32 [128], replicated, may hold values from 0.1 to 1.9
- factors: bfloat16 [2048, 2, 256], P('fs'), may hold values from -0.375 to 0.375
- moments: float32 [256, 2, 2048], P('fs', None, 'tp'), may hold values from -6 to 6
- weights: float32 [2048, 2, 2048], P('fs', None, 'tp'), may hold values from -6 to 6
Outputs:
- step: float32 [2048, 2, 2048], P('fs', None, 'tp')
- new_moments: float32 [256, 2, 2048], P('fs', None, 'tp')
- copies: bfloat16 [2048, 2, 2048], P(None, None, 'tp')
The draws below stay inside these ranges and needn't reach their ends.
All inputs are finite; a program needn't handle non-finite values.
Results may differ from the reference program's by a relative error of at most 0.007.
Values may be sent and summed in bfloat16 or wider, within the bound.
No kernel may reach another device: no remote copies, remote signals or barrier semaphores. Data moves between devices by JAX's collectives and lax.ppermute only.
A program may use at most 64 MiB of HBM per device.

```python
import jax
import jax.numpy as jnp
from jax import lax

D = 2048
HEADS = 16
HEAD_DIM = 64
RANK = 256
TOK_DEV = 384
HV = 2048
TOKENS = 24576


def pair_draw(key):
    shape = (TOKENS, HV)
    first_key, second_key = jax.random.split(jax.random.fold_in(key, 17), 2)
    query_vals = jnp.clip(jax.random.normal(first_key, shape, jnp.float32) * 1.3, -6.0, 6.0)
    key_vals = jnp.clip(jax.random.normal(second_key, shape, jnp.float32) * 1.3, -6.0, 6.0)
    return (query_vals, key_vals)


def draw_queries(key, part):
    return pair_draw(key)[0].astype(jnp.bfloat16)


def draw_keys(key, part):
    return pair_draw(key)[1].astype(jnp.bfloat16)


def steps_of(key, shape, cuts, low, largest):
    gain = 1.0
    for position, shards_of in cuts:
        heights = jax.random.uniform(jax.random.fold_in(jax.random.fold_in(key, 6), position), (shards_of,), jnp.float32, low / len(cuts), largest / len(cuts))
        gain = gain * jnp.repeat(jnp.exp(heights), shape[position] // shards_of).reshape((-1,) + (1,) * (len(shape) - 1 - position))
    return gain


def bell_draw(stream_key, shape, deviation, reach, cuts=(), kind=jnp.bfloat16):
    result = deviation * jax.random.normal(stream_key, shape, jnp.float32)
    if cuts:
        result = result * steps_of(stream_key, shape, cuts, -0.22, 0.18)
    return jnp.clip(result, -reach, reach).astype(kind)


def setup_inputs(seed: int = 0) -> dict:
    splits = jax.random.split(jax.random.key(seed), 11)
    return {
        "inputs": bell_draw(splits[0], (TOKENS, D), 1.0, 6.0, ((0, 64),)),
        "queries": draw_queries(jax.random.fold_in(splits[10], 71), 0),
        "keys": draw_keys(jax.random.fold_in(splits[10], 71), 0),
        "values": bell_draw(splits[3], (TOKENS, HV), 1.0, 6.0, ((0, 64), (1, 4))),
        "head_cot": bell_draw(splits[4], (TOKENS, HV), 1.0, 6.0, ((0, 64), (1, 4))),
        "mixing": jnp.clip(0.3 + 0.5 * jax.random.uniform(splits[5], (HEADS,), jnp.float32) ** steps_of(splits[5], (HEADS,), ((0, 4),), -0.2, 0.2), 0.3, 0.8),
        "head_gain": jnp.clip(1.0 + 0.18 * jax.random.normal(splits[6], (2 * HEAD_DIM,), jnp.float32), 0.1, 1.9),
        "factors": bell_draw(splits[7], (D, 2, RANK), RANK ** -0.5, 0.375, ((0, 64),)),
        "moments": bell_draw(splits[8], (RANK, 2, HV), 1.0, 6.0, ((0, 64), (2, 4)), jnp.float32),
        "weights": bell_draw(splits[9], (D, 2, HV), 1.0, 6.0, ((0, 64), (2, 4)), jnp.float32),
    }


EPS = 0.05
BETA = 0.9
RATE_BASE = 0.5

def softmax_rows(scores):
    top = lax.optimization_barrier(jnp.max(scores, axis=-1, keepdims=True))
    expo = jnp.exp(scores - top)
    return expo / lax.optimization_barrier(jnp.sum(expo, axis=-1, keepdims=True))

def head_grads(query, key_rows, value, upstream, weight_mix, head_gain):
    length = query.shape[0]
    head_dim = query.shape[2]
    factor = head_dim ** (-0.5)
    places = jnp.arange(length)
    causal = places[None, :] <= places[:, None]

    def probs(which):
        scores = jnp.dot(query[:, which], key_rows[:, which].T, preferred_element_type=jnp.float32) * factor
        return softmax_rows(jnp.where(causal, scores, -jnp.inf))
    first = probs(0)
    second = probs(1)
    mixed = (first - weight_mix * second).astype(jnp.bfloat16)
    output = jnp.dot(mixed, value, preferred_element_type=jnp.float32)
    inverse = lax.rsqrt(lax.optimization_barrier(jnp.mean(output * output, axis=-1, keepdims=True)) + EPS)
    scaled = head_gain * upstream.astype(jnp.float32)
    d_out = inverse * scaled - output * inverse ** 3 * lax.optimization_barrier(jnp.mean(output * scaled, axis=-1, keepdims=True))
    d_out = d_out.astype(jnp.bfloat16)
    d_value = jnp.dot(mixed.T, d_out, preferred_element_type=jnp.float32).astype(jnp.bfloat16)
    d_mix = jnp.dot(d_out, value.T, preferred_element_type=jnp.float32)
    d_first = (first * (d_mix - lax.optimization_barrier(jnp.sum(first * d_mix, axis=-1, keepdims=True)))).astype(jnp.bfloat16)
    d_second = (-weight_mix * second * (d_mix - lax.optimization_barrier(jnp.sum(second * d_mix, axis=-1, keepdims=True)))).astype(jnp.bfloat16)
    q_first = (jnp.dot(d_first, key_rows[:, 0], preferred_element_type=jnp.float32) * factor).astype(jnp.bfloat16)
    q_second = (jnp.dot(d_second, key_rows[:, 1], preferred_element_type=jnp.float32) * factor).astype(jnp.bfloat16)
    return (jnp.stack([q_first, q_second], axis=1).reshape(length, 2 * head_dim), d_value)

def reference(inputs, queries, keys, values, head_cot, mixing, head_gain, factors, moments, weights):
    sequences = TOKENS // TOK_DEV
    query_all = queries.reshape(sequences, TOK_DEV, HEADS, 2, HEAD_DIM)
    key_all = keys.reshape(sequences, TOK_DEV, HEADS, 2, HEAD_DIM)
    value_all = values.reshape(sequences, TOK_DEV, HEADS, 2 * HEAD_DIM)
    upstream_all = head_cot.reshape(sequences, TOK_DEV, HEADS, 2 * HEAD_DIM)
    per_head = jax.vmap(head_grads, in_axes=(1, 1, 1, 1, 0, None))

    def one_sequence(pieces):
        return per_head(pieces[0], pieces[1], pieces[2], pieces[3], mixing, head_gain)
    d_query, d_value = lax.map(one_sequence, (query_all, key_all, value_all, upstream_all))
    d_query = d_query.transpose(0, 2, 1, 3).reshape(TOKENS, HV)
    d_value = d_value.transpose(0, 2, 1, 3).reshape(TOKENS, HV)
    cotangents = jnp.stack([d_query, d_value], axis=1).reshape(TOKENS, 2 * HV)
    grads = jnp.dot(inputs.T, cotangents, preferred_element_type=jnp.float32).reshape(D, 2, HV)
    grads = grads * TOKENS ** (-0.5)
    factor_wide = factors.astype(jnp.float32)
    projected = jnp.einsum('dkr,dke->rke', factor_wide, grads, precision=lax.Precision.HIGHEST)
    new_moments = BETA * moments + projected
    totals = lax.optimization_barrier(jnp.sum(new_moments * new_moments, axis=(0, 2)))
    rate = RATE_BASE / jnp.sqrt(1.0 + totals / (RANK * HV))
    step = jnp.einsum('dkr,rke->dke', factor_wide, new_moments, precision=lax.Precision.HIGHEST) * rate[None, :, None]
    copies = (weights - step).astype(jnp.bfloat16)
    return (step, new_moments, copies)
```

```python
import jax
import jax.numpy as jnp
from jax import lax
from jax.sharding import Mesh
from jax.sharding import PartitionSpec as P

FS = ("fs_0", "fs_1", "fs_2")
FS_TP = ("fs_0", "fs_1", "fs_2", "tp")


EPS = 0.05
BETA = 0.9
RATE_BASE = 0.5


def sent_to_all(shard, axis):
    copies = jnp.broadcast_to(shard, (lax.axis_size(axis), *shard.shape))
    return lax.all_to_all(copies, axis, split_axis=0, concat_axis=0, tiled=True)


def joined_along(parts, dim):
    parts = jnp.moveaxis(parts, 0, dim)
    lengths = parts.shape
    return parts.reshape(*lengths[:dim], lengths[dim] * lengths[dim + 1], *lengths[dim + 2 :])


def collect(shard, axis, dim):
    parts = sent_to_all(shard, axis)
    return joined_along(parts, dim)


def in_blocks(shard, dim, length):
    lengths = shard.shape
    parts = shard.reshape(*lengths[:dim], length, lengths[dim] // length, *lengths[dim + 1 :])
    return jnp.moveaxis(parts, dim, 0)


def sum_at_owner(shard, axis, dim):
    length = lax.axis_size(axis)
    parts = lax.all_to_all(in_blocks(shard, dim, length), axis, 0, 0, tiled=True)
    return jnp.sum(parts, axis=0)


def by_axis(shard, axes):
    for axis in axes:
        shard = lax.psum(shard, axis)
    return shard


def softmax_rows(scores):
    top = jnp.max(scores, axis=-1, keepdims=True)
    expo = jnp.exp(scores - top)
    return expo / jnp.sum(expo, axis=-1, keepdims=True)


def head_grads(query, key_rows, value, upstream, weight_mix, head_gain):
    length = query.shape[0]
    head_dim = query.shape[2]
    factor = head_dim ** (-0.5)
    places = jnp.arange(length)
    causal = places[None, :] <= places[:, None]

    def probs(which):
        scores = (
            jnp.dot(query[:, which], key_rows[:, which].T, preferred_element_type=jnp.float32)
            * factor
        )
        return softmax_rows(jnp.where(causal, scores, -jnp.inf))

    first = probs(0)
    second = probs(1)
    mixed = (first - weight_mix * second).astype(jnp.bfloat16)
    output = jnp.dot(mixed, value, preferred_element_type=jnp.float32)
    inverse = lax.rsqrt(jnp.mean(output * output, axis=-1, keepdims=True) + EPS)
    scaled = head_gain * upstream.astype(jnp.float32)
    d_out = inverse * scaled - output * inverse**3 * jnp.mean(
        output * scaled, axis=-1, keepdims=True
    )
    d_out = d_out.astype(jnp.bfloat16)
    d_value = jnp.dot(mixed.T, d_out, preferred_element_type=jnp.float32).astype(jnp.bfloat16)
    d_mix = jnp.dot(d_out, value.T, preferred_element_type=jnp.float32)
    d_first = (first * (d_mix - jnp.sum(first * d_mix, axis=-1, keepdims=True))).astype(
        jnp.bfloat16
    )
    d_second = (
        -weight_mix * second * (d_mix - jnp.sum(second * d_mix, axis=-1, keepdims=True))
    ).astype(jnp.bfloat16)
    q_first = (
        jnp.dot(d_first, key_rows[:, 0], preferred_element_type=jnp.float32) * factor
    ).astype(jnp.bfloat16)
    q_second = (
        jnp.dot(d_second, key_rows[:, 1], preferred_element_type=jnp.float32) * factor
    ).astype(jnp.bfloat16)
    return (jnp.stack([q_first, q_second], axis=1).reshape(length, 2 * head_dim), d_value)


def per_device(
    inputs, queries, keys, values, head_cot, mixing, head_gain, factors, moments, weights
):
    length = inputs.shape[0]
    heads_here = mixing.shape[0]
    head_width = values.shape[1] // heads_here
    head_dim = head_width // 2
    query_heads = queries.reshape(length, heads_here, 2, head_dim).transpose(1, 0, 2, 3)
    key_heads = keys.reshape(length, heads_here, 2, head_dim).transpose(1, 0, 2, 3)
    value_heads = values.reshape(length, heads_here, head_width).transpose(1, 0, 2)
    upstream_heads = head_cot.reshape(length, heads_here, head_width).transpose(1, 0, 2)

    def one_head(pieces):
        return head_grads(pieces[0], pieces[1], pieces[2], pieces[3], pieces[4], head_gain)

    d_query, d_value = lax.map(
        one_head, (query_heads, key_heads, value_heads, upstream_heads, mixing)
    )
    d_query = d_query.transpose(1, 0, 2).reshape(length, heads_here * head_width)
    d_value = d_value.transpose(1, 0, 2).reshape(length, heads_here * head_width)
    cotangents = jnp.stack([d_query, d_value], axis=1)
    fs_count = lax.axis_size(FS)
    token_factor = (length * fs_count) ** (-0.5)
    rank_here = moments.shape[0]
    cols_here = moments.shape[2]
    whole_weights = lax.all_gather(weights.astype(jnp.bfloat16), FS, axis=0, tiled=True)
    whole_factors = collect(factors, FS, 0)
    reduced = jnp.einsum("td,dkr->tkr", inputs, whole_factors, preferred_element_type=jnp.float32)
    reduced_upper = reduced.astype(jnp.bfloat16)
    reduced_lower = (reduced - reduced_upper.astype(jnp.float32)).astype(jnp.bfloat16)
    upper_part = jnp.einsum(
        "tkr,tke->rke", reduced_upper, cotangents, preferred_element_type=jnp.float32
    )
    lower_part = jnp.einsum(
        "tkr,tke->rke", reduced_lower, cotangents, preferred_element_type=jnp.float32
    )
    partial = ((upper_part + lower_part) * token_factor).astype(jnp.bfloat16)
    parts = lax.all_to_all(in_blocks(partial, 0, fs_count), FS, 0, 0, tiled=True)
    projected = jnp.sum(parts.astype(jnp.float32), axis=0)
    new_moments = BETA * moments + projected
    whole_moments = collect(new_moments.astype(jnp.bfloat16), FS, 0)
    wide_moments = whole_moments.astype(jnp.float32)
    totals = lax.psum(jnp.sum(wide_moments * wide_moments, axis=(0, 2)), "tp")
    entries = rank_here * fs_count * cols_here * lax.axis_size("tp")
    rate = RATE_BASE / jnp.sqrt(1.0 + totals / entries)
    own_part = jnp.einsum(
        "dkr,rke->dke", factors, whole_moments, preferred_element_type=jnp.float32
    )
    step = own_part * rate[None, :, None]
    low_part = jnp.einsum(
        "dkr,rke->dke", whole_factors, whole_moments, preferred_element_type=jnp.float32
    )
    copies = (whole_weights.astype(jnp.float32) - low_part * rate[None, :, None]).astype(
        jnp.bfloat16
    )
    return (step, new_moments, copies)


def solution(mesh):
    torus = Mesh(mesh.devices.reshape(8, 4, 2, mesh.shape["tp"]), ("fs_0", "fs_1", "fs_2", "tp"))
    placed = (
        P(FS, None),
        P(FS, "tp"),
        P(FS, "tp"),
        P(FS, "tp"),
        P(FS, "tp"),
        P("tp"),
        P(),
        P(FS, None, None),
        P(FS, None, "tp"),
        P(FS, None, "tp"),
    )
    return jax.shard_map(
        per_device,
        mesh=torus,
        in_specs=placed,
        out_specs=(P(FS, None, "tp"), P(FS, None, "tp"), P(None, None, "tp")),
        check_vma=False,
    )
```

```python
import functools

import jax
import jax.numpy as jnp
from jax import lax
from jax.experimental import pallas as pl
from jax.experimental.pallas import tpu as pltpu
from jax.sharding import Mesh
from jax.sharding import PartitionSpec as P

PLANE = ("fs_0", "fs_1")
CORE = "fs_2"
FS = (*PLANE, CORE)

EPS = 0.05
BETA = 0.9
RATE_BASE = 0.5
BF16 = jnp.bfloat16
F32 = jnp.float32


def nt_dot(left, right):
    return lax.dot_general(left, right, (((1,), (1,)), ((), ())), preferred_element_type=F32)


def tn_dot(left, right):
    return lax.dot_general(left, right, (((0,), (0,)), ((), ())), preferred_element_type=F32)


def attention_kernel(rows, mix_ref, q_ref, k_ref, v_ref, up_ref, gain_ref, dq_ref, dv_ref, sum_ref):
    length, width = q_ref.shape
    head_dim = width // 2
    factor = head_dim**-0.5
    weight_mix = mix_ref[pl.program_id(0)]
    gain = gain_ref[...]
    for start in range(0, length, rows):
        seen = start + rows
        query = q_ref[start:seen, :]
        keys = k_ref[:seen, :]
        value = v_ref[:seen, :]
        place = lax.broadcasted_iota(jnp.int32, (rows, seen), 0) + start
        causal = lax.broadcasted_iota(jnp.int32, (rows, seen), 1) <= place

        def probs(which):
            cols = slice(which * head_dim, (which + 1) * head_dim)
            scores = nt_dot(query[:, cols], keys[:, cols]) * factor
            scores = jnp.where(causal, scores, -jnp.inf)
            expo = jnp.exp(scores - jnp.max(scores, axis=-1, keepdims=True))
            return expo * (1.0 / jnp.sum(expo, axis=-1, keepdims=True))

        first = probs(0)
        second = weight_mix * probs(1)
        mixed = (first - second).astype(BF16)
        output = jnp.dot(mixed, value, preferred_element_type=F32)
        inverse = lax.rsqrt(jnp.mean(output * output, axis=-1, keepdims=True) + EPS)
        scaled = gain * up_ref[start:seen, :].astype(F32)
        along = jnp.mean(output * scaled, axis=-1, keepdims=True)
        d_out = (inverse * scaled - output * (inverse * inverse * inverse * along)).astype(BF16)
        d_value = tn_dot(mixed, d_out)
        if start:
            sum_ref[:start, :] += d_value[:start]
        sum_ref[start:seen, :] = d_value[start:]
        d_mix = nt_dot(d_out, value)
        first_mix = jnp.sum(first * d_mix, axis=-1, keepdims=True)
        second_mix = jnp.sum(second * d_mix, axis=-1, keepdims=True) * (1.0 / weight_mix)
        d_first = (first * (d_mix - first_mix)).astype(BF16)
        d_second = (second * (second_mix - d_mix)).astype(BF16)
        dq_ref[start:seen, :head_dim] = (
            jnp.dot(d_first, keys[:, :head_dim], preferred_element_type=F32) * factor
        ).astype(BF16)
        dq_ref[start:seen, head_dim:] = (
            jnp.dot(d_second, keys[:, head_dim:], preferred_element_type=F32) * factor
        ).astype(BF16)
    dv_ref[...] = sum_ref[...].astype(BF16)


def attention_grads(queries, keys, values, head_cot, mixing, head_gain, rows=128):
    length, cols = queries.shape
    heads = mixing.shape[0]
    width = cols // heads
    block = pl.BlockSpec((length, width), lambda h: (0, h))
    return pl.pallas_call(
        functools.partial(attention_kernel, rows),
        grid=(heads,),
        in_specs=[
            pl.BlockSpec(memory_space=pltpu.SMEM),
            block,
            block,
            block,
            block,
            pl.BlockSpec((1, width), lambda h: (0, 0)),
        ],
        out_specs=[block, block],
        out_shape=[jax.ShapeDtypeStruct((length, cols), BF16)] * 2,
        scratch_shapes=[pltpu.VMEM((length, width), F32)],
        cost_estimate=pl.CostEstimate(
            flops=20 * length * length * cols,
            transcendentals=2 * heads * length * length,
            bytes_accessed=12 * length * cols,
        ),
        name="attention_grads",
    )(mixing, queries, keys, values, head_cot, head_gain.reshape(1, width))


def low_rank_rows(scale_ref, factor_rows, moment_ref, rows_ref):
    maps, rank, cols = moment_ref.shape
    count = factor_rows.shape[0]
    tiles = cols // 128
    for k in range(maps):
        part = jnp.dot(
            factor_rows[:, k * rank : (k + 1) * rank], moment_ref[k], preferred_element_type=F32
        )
        part = part * scale_ref[k]
        for j in range(tiles):
            rows_ref[pl.ds(maps * j + k, count, stride=maps * tiles), :] = part[
                :, j * 128 : (j + 1) * 128
            ]


def update_kernel(scale_ref, own_ref, factor_ref, moment_ref, weight_ref, step_ref, copy_ref, rows_ref):
    @pl.when(pl.program_id(0) == 0)
    def _():
        low_rank_rows(scale_ref, own_ref[...], moment_ref, step_ref)

    low_rank_rows(scale_ref, factor_ref[...], moment_ref, rows_ref)
    copy_ref[...] = (weight_ref[...].astype(F32) - rows_ref[...]).astype(BF16)


def update(rate, own_factors, whole_factors, whole_moments, whole_weights, rows=256):
    depth, width = whole_factors.shape
    own_depth = own_factors.shape[0]
    maps, rank, cols = whole_moments.shape
    each = maps * cols // 128
    return pl.pallas_call(
        update_kernel,
        grid=(depth // rows,),
        in_specs=[
            pl.BlockSpec(memory_space=pltpu.SMEM),
            pl.BlockSpec((own_depth, width), lambda i: (0, 0)),
            pl.BlockSpec((rows, width), lambda i: (i, 0)),
            pl.BlockSpec((maps, rank, cols), lambda i: (0, 0, 0)),
            pl.BlockSpec((rows * each, 128), lambda i: (i, 0)),
        ],
        out_specs=[
            pl.BlockSpec((own_depth * each, 128), lambda i: (0, 0)),
            pl.BlockSpec((rows * each, 128), lambda i: (i, 0)),
        ],
        out_shape=[
            jax.ShapeDtypeStruct((own_depth * each, 128), F32),
            jax.ShapeDtypeStruct((depth * each, 128), BF16),
        ],
        scratch_shapes=[pltpu.VMEM((rows * each, 128), F32)],
        cost_estimate=pl.CostEstimate(
            flops=2 * depth * maps * rank * cols,
            transcendentals=0,
            bytes_accessed=2 * depth * width + 4 * depth * maps * cols,
        ),
        name="low_rank_update",
    )(rate, own_factors, whole_factors, whole_moments, whole_weights)


def as_rows(array):
    depth, maps, cols = array.shape
    tiles = array.reshape(depth, maps, cols // 128, 128).transpose(0, 2, 1, 3)
    return tiles.reshape(depth * maps * cols // 128, 128)


def from_rows(rows, maps, cols):
    tiles = rows.reshape(-1, cols // 128, maps, 128).transpose(0, 2, 1, 3)
    return tiles.reshape(-1, maps, cols)


def sent_to_all(shard, axis):
    copies = jnp.broadcast_to(shard, (lax.axis_size(axis), *shard.shape))
    return lax.all_to_all(copies, axis, split_axis=0, concat_axis=0, tiled=True)


def gather_rows(shard, beside):
    mine, beside = lax.optimization_barrier((sent_to_all(shard, PLANE), beside))
    other = lax.ppermute(mine, CORE, [(0, 1), (1, 0)])
    low = lax.axis_index(CORE) == 0
    both = jnp.stack([jnp.where(low, mine, other), jnp.where(low, other, mine)], axis=1)
    return both.reshape(-1, *shard.shape[1:]), beside


def per_device(
    inputs, queries, keys, values, head_cot, mixing, head_gain, factors, moments, weights
):
    length = inputs.shape[0]
    fs_count = lax.axis_size(FS)
    token_factor = (length * fs_count) ** (-0.5)
    rank_here, maps, cols = moments.shape
    rank = rank_here * fs_count
    whole_weights = lax.all_gather(as_rows(weights).astype(BF16), FS, axis=0, tiled=True)
    own_factors = factors.reshape(-1, maps * rank)
    cotangents = attention_grads(queries, keys, values, head_cot, mixing, head_gain)
    whole_factors, cotangents = gather_rows(own_factors, cotangents)
    reduced = jnp.dot(inputs, whole_factors, preferred_element_type=F32)
    upper = reduced.astype(BF16)
    lower = (reduced - upper.astype(F32)).astype(BF16)
    partial = jnp.stack(
        [
            tn_dot(upper[:, k * rank : (k + 1) * rank], cotangents[k])
            + tn_dot(lower[:, k * rank : (k + 1) * rank], cotangents[k])
            for k in range(maps)
        ]
    )
    partial = (partial * token_factor).astype(BF16).reshape(maps, fs_count, rank_here, cols)
    partial = partial.transpose(1, 0, 2, 3).reshape(fs_count, maps * rank_here, cols)
    parts = lax.all_to_all(partial, FS, 0, 0, tiled=True)
    projected = jnp.sum(parts.astype(F32), axis=0).reshape(maps, rank_here, cols)
    new_moments = BETA * moments + projected.transpose(1, 0, 2)
    sent = new_moments.astype(BF16).transpose(1, 0, 2).reshape(maps * rank_here, cols)
    whole_moments = sent_to_all(sent, FS).reshape(fs_count, maps, rank_here, cols)
    whole_moments = whole_moments.transpose(1, 0, 2, 3).reshape(maps, rank, cols)
    wide = whole_moments.astype(F32)
    totals = lax.psum(jnp.sum(wide * wide, axis=(1, 2)), "tp")
    rate = RATE_BASE / jnp.sqrt(1.0 + totals / (rank * cols * lax.axis_size("tp")))
    step, copies = update(rate, own_factors, whole_factors, whole_moments, whole_weights)
    return (from_rows(step, maps, cols), new_moments, from_rows(copies, maps, cols))


def solution(mesh):
    torus = Mesh(mesh.devices.reshape(8, 4, 2, mesh.shape["tp"]), (*FS, "tp"))
    placed = (
        P(FS, None),
        P(FS, "tp"),
        P(FS, "tp"),
        P(FS, "tp"),
        P(FS, "tp"),
        P("tp"),
        P(),
        P(FS, None, None),
        P(FS, None, "tp"),
        P(FS, None, "tp"),
    )
    return jax.shard_map(
        per_device,
        mesh=torus,
        in_specs=placed,
        out_specs=(P(FS, None, "tp"), P(FS, None, "tp"), P(None, None, "tp")),
        check_vma=False,
    )
```

```python
import functools

import jax
import jax.numpy as jnp
from jax import lax
from jax.experimental import pallas as pl
from jax.experimental.pallas import tpu as pltpu
from jax.sharding import Mesh
from jax.sharding import PartitionSpec as P

DEEP, WIDE, CORE = "fs_0", "fs_1", "fs_2"
PLANE = (DEEP, WIDE)
FS = (*PLANE, CORE)
SWAP = [(0, 1), (1, 0)]

EPS = 0.05
BETA = 0.9
RATE_BASE = 0.5
BF16 = jnp.bfloat16
F32 = jnp.float32


def nt_dot(left, right):
    return lax.dot_general(left, right, (((1,), (1,)), ((), ())), preferred_element_type=F32)


def tn_dot(left, right):
    return lax.dot_general(left, right, (((0,), (0,)), ((), ())), preferred_element_type=F32)


def attention_kernel(rows, mix_ref, q_ref, k_ref, v_ref, up_ref, gain_ref, dq_ref, dv_ref, sum_ref):
    length, width = q_ref.shape
    head_dim = width // 2
    factor = head_dim**-0.5
    weight_mix = mix_ref[pl.program_id(0)]
    gain = gain_ref[...]
    for start in range(0, length, rows):
        seen = start + rows
        query = q_ref[start:seen, :]
        keys = k_ref[:seen, :]
        value = v_ref[:seen, :]
        place = lax.broadcasted_iota(jnp.int32, (rows, seen), 0) + start
        causal = lax.broadcasted_iota(jnp.int32, (rows, seen), 1) <= place

        def probs(which):
            cols = slice(which * head_dim, (which + 1) * head_dim)
            scores = nt_dot(query[:, cols], keys[:, cols]) * factor
            scores = jnp.where(causal, scores, -jnp.inf)
            expo = jnp.exp(scores - jnp.max(scores, axis=-1, keepdims=True))
            return expo * (1.0 / jnp.sum(expo, axis=-1, keepdims=True))

        first = probs(0)
        second = weight_mix * probs(1)
        mixed = (first - second).astype(BF16)
        output = jnp.dot(mixed, value, preferred_element_type=F32)
        inverse = lax.rsqrt(jnp.mean(output * output, axis=-1, keepdims=True) + EPS)
        scaled = gain * up_ref[start:seen, :].astype(F32)
        along = jnp.mean(output * scaled, axis=-1, keepdims=True)
        d_out = (inverse * scaled - output * (inverse * inverse * inverse * along)).astype(BF16)
        d_value = tn_dot(mixed, d_out)
        if start:
            sum_ref[:start, :] += d_value[:start]
        sum_ref[start:seen, :] = d_value[start:]
        d_mix = nt_dot(d_out, value)
        first_mix = jnp.sum(first * d_mix, axis=-1, keepdims=True)
        second_mix = jnp.sum(second * d_mix, axis=-1, keepdims=True) * (1.0 / weight_mix)
        d_first = (first * (d_mix - first_mix)).astype(BF16)
        d_second = (second * (second_mix - d_mix)).astype(BF16)
        dq_ref[start:seen, :head_dim] = (
            jnp.dot(d_first, keys[:, :head_dim], preferred_element_type=F32) * factor
        ).astype(BF16)
        dq_ref[start:seen, head_dim:] = (
            jnp.dot(d_second, keys[:, head_dim:], preferred_element_type=F32) * factor
        ).astype(BF16)
    dv_ref[...] = sum_ref[...].astype(BF16)


def attention_grads(queries, keys, values, head_cot, mixing, head_gain, rows=128):
    length, cols = queries.shape
    heads = mixing.shape[0]
    width = cols // heads
    block = pl.BlockSpec((length, width), lambda h: (0, h))
    return pl.pallas_call(
        functools.partial(attention_kernel, rows),
        grid=(heads,),
        in_specs=[
            pl.BlockSpec(memory_space=pltpu.SMEM),
            block,
            block,
            block,
            block,
            pl.BlockSpec((1, width), lambda h: (0, 0)),
        ],
        out_specs=[block, block],
        out_shape=[jax.ShapeDtypeStruct((length, cols), BF16)] * 2,
        scratch_shapes=[pltpu.VMEM((length, width), F32)],
        cost_estimate=pl.CostEstimate(
            flops=20 * length * length * cols,
            transcendentals=2 * heads * length * length,
            bytes_accessed=12 * length * cols,
        ),
        name="attention_grads",
    )(mixing, queries, keys, values, head_cot, head_gain.reshape(1, width))


def interleaved(first, second):
    half = lax.broadcasted_iota(jnp.int32, first.shape, 0) % 8 < 4
    count = first.shape[0]
    even = jnp.where(half, first, pltpu.roll(second, 4, 0))
    odd = jnp.where(half, pltpu.roll(first, count - 4, 0), second)
    return even, odd


def separated(even, odd):
    half = lax.broadcasted_iota(jnp.int32, even.shape, 0) % 8 < 4
    count = even.shape[0]
    first = jnp.where(half, even, pltpu.roll(odd, 4, 0))
    second = jnp.where(half, pltpu.roll(even, count - 4, 0), odd)
    return first, second


def fill_rows(low, mine_ref, other_ref, rows_ref):
    xs, zs, rows, _ = mine_ref.shape
    for z in range(zs):
        for x in range(xs):
            mine, other = mine_ref[x, z], other_ref[x, z]
            at = 2 * rows * (z * xs + x)
            rows_ref[at : at + rows, :] = jnp.where(low, mine, other)
            rows_ref[at + rows : at + 2 * rows, :] = jnp.where(low, other, mine)


def project_kernel(
    scale, core_ref, mine_ref, other_ref, in_ref, dq_ref, dv_ref, keep_ref, send_ref, rows_ref, red_ref
):
    step = pl.program_id(0)
    low = core_ref[0] == 0
    fill_rows(low, mine_ref, other_ref, rows_ref)
    part = jnp.dot(in_ref[...], rows_ref[...], preferred_element_type=F32)

    @pl.when(step == 0)
    def _():
        red_ref[...] = part

    @pl.when(step > 0)
    def _():
        red_ref[...] += part

    @pl.when(step == pl.num_programs(0) - 1)
    def _():
        reduced = red_ref[...]
        upper = reduced.astype(BF16)
        lower = (reduced - upper.astype(F32)).astype(BF16)
        rank = keep_ref.shape[0]
        sums = []
        for k, cot_ref in enumerate((dq_ref, dv_ref)):
            cols = slice(k * rank, (k + 1) * rank)
            cot = cot_ref[...]
            sums.append((tn_dot(upper[:, cols], cot) + tn_dot(lower[:, cols], cot)) * scale)
        even, odd = interleaved(*sums)
        keep_ref[...] = jnp.where(low, even, odd)
        send_ref[...] = jnp.where(low, odd, even)


def project(scale, core, mine, other, inputs, d_query, d_value, each=2):
    xs, zs, rows, width = mine.shape
    length, depth = inputs.shape
    cols = d_query.shape[1]
    rank = width // 2
    block = pl.BlockSpec((xs, each, rows, width), lambda i: (0, i, 0, 0))
    span = 2 * xs * each * rows
    whole = pl.BlockSpec((length, cols), lambda i: (0, 0))
    result = pl.BlockSpec((rank, cols), lambda i: (0, 0))
    return pl.pallas_call(
        functools.partial(project_kernel, scale),
        grid=(zs // each,),
        in_specs=[
            pl.BlockSpec(memory_space=pltpu.SMEM),
            block,
            block,
            pl.BlockSpec((length, span), lambda i: (0, i)),
            whole,
            whole,
        ],
        out_specs=[result, result],
        out_shape=[jax.ShapeDtypeStruct((rank, cols), F32)] * 2,
        scratch_shapes=[pltpu.VMEM((span, width), BF16), pltpu.VMEM((length, width), F32)],
        cost_estimate=pl.CostEstimate(
            flops=2 * length * width * (depth + 2 * cols),
            transcendentals=0,
            bytes_accessed=2 * depth * (length + width) + 4 * length * cols + 8 * rank * cols,
        ),
        name="project",
    )(core, mine, other, inputs, d_query, d_value)


def low_rank_rows(scale_ref, factor_rows, moment_ref, rows_ref):
    maps, rank, cols = moment_ref.shape
    count = factor_rows.shape[0]
    tiles = cols // 128
    for k in range(maps):
        part = jnp.dot(
            factor_rows[:, k * rank : (k + 1) * rank], moment_ref[k], preferred_element_type=F32
        )
        part = part * scale_ref[k]
        for j in range(tiles):
            rows_ref[pl.ds(maps * j + k, count, stride=maps * tiles), :] = part[
                :, j * 128 : (j + 1) * 128
            ]


def update_kernel(
    core_ref,
    scale_ref,
    own_ref,
    mine_ref,
    other_ref,
    moment_mine_ref,
    moment_other_ref,
    weight_ref,
    step_ref,
    copy_ref,
    factor_ref,
    moment_ref,
    rows_ref,
):
    low = core_ref[0] == 0

    @pl.when(pl.program_id(0) == 0)
    def _():
        mine = moment_mine_ref[...].astype(F32)
        other = moment_other_ref[...].astype(F32)
        first, second = separated(jnp.where(low, mine, other), jnp.where(low, other, mine))
        moment_ref[0] = first.astype(BF16)
        moment_ref[1] = second.astype(BF16)
        low_rank_rows(scale_ref, own_ref[...], moment_ref, step_ref)

    fill_rows(low, mine_ref, other_ref, factor_ref)
    low_rank_rows(scale_ref, factor_ref[...], moment_ref, rows_ref)
    copy_ref[...] = (weight_ref[...].astype(F32) - rows_ref[...]).astype(BF16)


def update(core, rate, own_factors, mine, other, moments_mine, moments_other, whole_weights):
    xs, zs, rows, width = mine.shape
    rank, cols = moments_mine.shape
    maps = width // rank
    each = maps * cols // 128
    span = 2 * xs * rows
    depth = span * zs
    own_depth = own_factors.shape[0]
    block = pl.BlockSpec((xs, 1, rows, width), lambda i: (0, i, 0, 0))
    moment_block = pl.BlockSpec((rank, cols), lambda i: (0, 0))
    return pl.pallas_call(
        update_kernel,
        grid=(zs,),
        in_specs=[
            pl.BlockSpec(memory_space=pltpu.SMEM),
            pl.BlockSpec(memory_space=pltpu.SMEM),
            pl.BlockSpec((own_depth, width), lambda i: (0, 0)),
            block,
            block,
            moment_block,
            moment_block,
            pl.BlockSpec((span * each, 128), lambda i: (i, 0)),
        ],
        out_specs=[
            pl.BlockSpec((own_depth * each, 128), lambda i: (0, 0)),
            pl.BlockSpec((span * each, 128), lambda i: (i, 0)),
        ],
        out_shape=[
            jax.ShapeDtypeStruct((own_depth * each, 128), F32),
            jax.ShapeDtypeStruct((depth * each, 128), BF16),
        ],
        scratch_shapes=[
            pltpu.VMEM((span, width), BF16),
            pltpu.VMEM((maps, rank, cols), BF16),
            pltpu.VMEM((span * each, 128), F32),
        ],
        cost_estimate=pl.CostEstimate(
            flops=2 * depth * width * cols,
            transcendentals=0,
            bytes_accessed=2 * depth * width + 4 * depth * maps * cols,
        ),
        name="low_rank_update",
    )(core, rate, own_factors, mine, other, moments_mine, moments_other, whole_weights)


def as_rows(array):
    depth, maps, cols = array.shape
    tiles = array.reshape(depth, maps, cols // 128, 128).transpose(0, 2, 1, 3)
    return tiles.reshape(depth * maps * cols // 128, 128)


def from_rows(rows, maps, cols):
    tiles = rows.reshape(-1, cols // 128, maps, 128).transpose(0, 2, 1, 3)
    return tiles.reshape(-1, maps, cols)


def sent_to_all(shard, axis):
    copies = jnp.broadcast_to(shard, (lax.axis_size(axis), *shard.shape))
    return lax.all_to_all(copies, axis, split_axis=0, concat_axis=0, tiled=True)


def per_device(
    inputs, queries, keys, values, head_cot, mixing, head_gain, factors, moments, weights
):
    length = inputs.shape[0]
    planes = lax.axis_size(PLANE)
    fs_count = lax.axis_size(FS)
    token_factor = (length * fs_count) ** (-0.5)
    rank_here, maps, cols = moments.shape
    rank = rank_here * fs_count
    core = lax.axis_index(CORE).reshape(1)
    own_factors = factors.reshape(-1, maps * rank)
    columns = sent_to_all(own_factors, DEEP)
    columns, weights = lax.optimization_barrier((columns, weights))
    whole_weights = lax.all_gather(as_rows(weights).astype(BF16), FS, axis=0, tiled=True)
    mine = sent_to_all(columns, WIDE)
    d_query, d_value = attention_grads(queries, keys, values, head_cot, mixing, head_gain)
    mine, d_query, d_value = lax.optimization_barrier((mine, d_query, d_value))
    other = lax.ppermute(mine, CORE, SWAP)
    keep, send = project(token_factor, core, mine, other, inputs, d_query, d_value)
    summed = (keep + lax.ppermute(send, CORE, SWAP)).astype(BF16)
    summed = summed.reshape(planes, maps * rank_here, cols)
    parts = lax.all_to_all(summed, PLANE, 0, 0, tiled=True)
    projected = jnp.sum(parts.astype(F32), axis=0).reshape(maps, rank_here, cols)
    new_moments = BETA * moments + projected.transpose(1, 0, 2)
    sent = new_moments.astype(BF16).transpose(1, 0, 2).reshape(maps * rank_here, cols)
    moments_mine = sent_to_all(sent, PLANE)
    moments_other = lax.ppermute(moments_mine, CORE, SWAP)
    squares = moments_mine.astype(F32) ** 2 + moments_other.astype(F32) ** 2
    squares = jnp.sum(squares.reshape(planes, maps, rank_here, cols), axis=(0, 2, 3))
    totals = lax.psum(squares, "tp")
    rate = RATE_BASE / jnp.sqrt(1.0 + totals / (rank * cols * lax.axis_size("tp")))
    step, copies = update(
        core,
        rate,
        own_factors,
        mine,
        other,
        moments_mine.reshape(rank, cols),
        moments_other.reshape(rank, cols),
        whole_weights,
    )
    return (from_rows(step, maps, cols), new_moments, from_rows(copies, maps, cols))


def solution(mesh):
    torus = Mesh(mesh.devices.reshape(8, 4, 2, mesh.shape["tp"]), (*FS, "tp"))
    placed = (
        P(FS, None),
        P(FS, "tp"),
        P(FS, "tp"),
        P(FS, "tp"),
        P(FS, "tp"),
        P("tp"),
        P(),
        P(FS, None, None),
        P(FS, None, "tp"),
        P(FS, None, "tp"),
    )
    return jax.shard_map(
        per_device,
        mesh=torus,
        in_specs=placed,
        out_specs=(P(FS, None, "tp"), P(FS, None, "tp"), P(None, None, "tp")),
        check_vma=False,
    )
```

```python
import functools

import jax
import jax.numpy as jnp
from jax import lax
from jax.experimental import pallas as pl
from jax.experimental.pallas import tpu as pltpu
from jax.sharding import Mesh
from jax.sharding import PartitionSpec as P

DEEP, WIDE, CORE = "fs_0", "fs_1", "fs_2"
PLANE = (DEEP, WIDE)
FS = (*PLANE, CORE)
SWAP = [(0, 1), (1, 0)]

EPS = 0.05
BETA = 0.9
RATE_BASE = 0.5
BF16 = jnp.bfloat16
F32 = jnp.float32


def nt_dot(left, right):
    return lax.dot_general(left, right, (((1,), (1,)), ((), ())), preferred_element_type=F32)


def tn_dot(left, right):
    return lax.dot_general(left, right, (((0,), (0,)), ((), ())), preferred_element_type=F32)


def attention_kernel(rows, mix_ref, q_ref, k_ref, v_ref, up_ref, gain_ref, dq_ref, dv_ref, sum_ref):
    length, width = q_ref.shape
    head_dim = width // 2
    factor = head_dim**-0.5
    weight_mix = mix_ref[pl.program_id(0)]
    gain = gain_ref[...]
    for start in range(0, length, rows):
        seen = start + rows
        query = q_ref[start:seen, :]
        keys = k_ref[:seen, :]
        value = v_ref[:seen, :]
        place = lax.broadcasted_iota(jnp.int32, (rows, seen), 0) + start
        causal = lax.broadcasted_iota(jnp.int32, (rows, seen), 1) <= place

        def probs(which):
            cols = slice(which * head_dim, (which + 1) * head_dim)
            scores = nt_dot(query[:, cols], keys[:, cols]) * factor
            scores = jnp.where(causal, scores, -jnp.inf)
            expo = jnp.exp(scores - jnp.max(scores, axis=-1, keepdims=True))
            return expo * (1.0 / jnp.sum(expo, axis=-1, keepdims=True))

        first = probs(0)
        second = weight_mix * probs(1)
        mixed = (first - second).astype(BF16)
        output = jnp.dot(mixed, value, preferred_element_type=F32)
        inverse = lax.rsqrt(jnp.mean(output * output, axis=-1, keepdims=True) + EPS)
        scaled = gain * up_ref[start:seen, :].astype(F32)
        along = jnp.mean(output * scaled, axis=-1, keepdims=True)
        d_out = (inverse * scaled - output * (inverse * inverse * inverse * along)).astype(BF16)
        d_value = tn_dot(mixed, d_out)
        if start:
            sum_ref[:start, :] += d_value[:start]
        sum_ref[start:seen, :] = d_value[start:]
        d_mix = nt_dot(d_out, value)
        first_mix = jnp.sum(first * d_mix, axis=-1, keepdims=True)
        second_mix = jnp.sum(second * d_mix, axis=-1, keepdims=True) * (1.0 / weight_mix)
        d_first = (first * (d_mix - first_mix)).astype(BF16)
        d_second = (second * (second_mix - d_mix)).astype(BF16)
        dq_ref[start:seen, :head_dim] = (
            jnp.dot(d_first, keys[:, :head_dim], preferred_element_type=F32) * factor
        ).astype(BF16)
        dq_ref[start:seen, head_dim:] = (
            jnp.dot(d_second, keys[:, head_dim:], preferred_element_type=F32) * factor
        ).astype(BF16)
    dv_ref[...] = sum_ref[...].astype(BF16)


def attention_grads(queries, keys, values, head_cot, mixing, head_gain, rows=384):
    length, cols = queries.shape
    heads = mixing.shape[0]
    width = cols // heads
    block = pl.BlockSpec((length, width), lambda h: (0, h))
    return pl.pallas_call(
        functools.partial(attention_kernel, rows),
        grid=(heads,),
        in_specs=[
            pl.BlockSpec(memory_space=pltpu.SMEM),
            block,
            block,
            block,
            block,
            pl.BlockSpec((1, width), lambda h: (0, 0)),
        ],
        out_specs=[block, block],
        out_shape=[jax.ShapeDtypeStruct((length, cols), BF16)] * 2,
        scratch_shapes=[pltpu.VMEM((length, width), F32)],
        cost_estimate=pl.CostEstimate(
            flops=20 * length * length * cols,
            transcendentals=2 * heads * length * length,
            bytes_accessed=12 * length * cols,
        ),
        name="attention_grads",
    )(mixing, queries, keys, values, head_cot, head_gain.reshape(1, width))


def interleaved(first, second):
    half = lax.broadcasted_iota(jnp.int32, first.shape, 0) % 8 < 4
    count = first.shape[0]
    even = jnp.where(half, first, pltpu.roll(second, 4, 0))
    odd = jnp.where(half, pltpu.roll(first, count - 4, 0), second)
    return even, odd


def separated(even, odd):
    half = lax.broadcasted_iota(jnp.int32, even.shape, 0) % 8 < 4
    count = even.shape[0]
    first = jnp.where(half, even, pltpu.roll(odd, 4, 0))
    second = jnp.where(half, pltpu.roll(even, count - 4, 0), odd)
    return first, second


def fill_rows(low, mine_ref, other_ref, rows_ref):
    xs, zs, rows, _ = mine_ref.shape
    for z in range(zs):
        for x in range(xs):
            mine, other = mine_ref[x, z], other_ref[x, z]
            at = 2 * rows * (z * xs + x)
            rows_ref[at : at + rows, :] = jnp.where(low, mine, other)
            rows_ref[at + rows : at + 2 * rows, :] = jnp.where(low, other, mine)


def project_kernel(
    scale, core_ref, mine_ref, other_ref, in_ref, dq_ref, dv_ref, keep_ref, send_ref, rows_ref, red_ref
):
    step = pl.program_id(0)
    low = core_ref[0] == 0
    fill_rows(low, mine_ref, other_ref, rows_ref)
    part = jnp.dot(in_ref[...], rows_ref[...], preferred_element_type=F32)

    @pl.when(step == 0)
    def _():
        red_ref[...] = part

    @pl.when(step > 0)
    def _():
        red_ref[...] += part

    @pl.when(step == pl.num_programs(0) - 1)
    def _():
        reduced = red_ref[...]
        upper = reduced.astype(BF16)
        lower = (reduced - upper.astype(F32)).astype(BF16)
        rank = keep_ref.shape[0]
        sums = []
        for k, cot_ref in enumerate((dq_ref, dv_ref)):
            cols = slice(k * rank, (k + 1) * rank)
            cot = cot_ref[...]
            sums.append((tn_dot(upper[:, cols], cot) + tn_dot(lower[:, cols], cot)) * scale)
        even, odd = interleaved(*sums)
        keep_ref[...] = jnp.where(low, even, odd)
        send_ref[...] = jnp.where(low, odd, even)


def project(scale, core, mine, other, inputs, d_query, d_value, each=4):
    xs, zs, rows, width = mine.shape
    length, depth = inputs.shape
    cols = d_query.shape[1]
    rank = width // 2
    block = pl.BlockSpec((xs, each, rows, width), lambda i: (0, i, 0, 0))
    span = 2 * xs * each * rows
    whole = pl.BlockSpec((length, cols), lambda i: (0, 0))
    result = pl.BlockSpec((rank, cols), lambda i: (0, 0))
    return pl.pallas_call(
        functools.partial(project_kernel, scale),
        grid=(zs // each,),
        in_specs=[
            pl.BlockSpec(memory_space=pltpu.SMEM),
            block,
            block,
            pl.BlockSpec((length, span), lambda i: (0, i)),
            whole,
            whole,
        ],
        out_specs=[result, result],
        out_shape=[jax.ShapeDtypeStruct((rank, cols), F32)] * 2,
        scratch_shapes=[pltpu.VMEM((span, width), BF16), pltpu.VMEM((length, width), F32)],
        cost_estimate=pl.CostEstimate(
            flops=2 * length * width * (depth + 2 * cols),
            transcendentals=0,
            bytes_accessed=2 * depth * (length + width) + 4 * length * cols + 8 * rank * cols,
        ),
        name="project",
    )(core, mine, other, inputs, d_query, d_value)


def low_rank_rows(scale_ref, factor_rows, moment_ref, rows_ref):
    maps, rank, cols = moment_ref.shape
    count = factor_rows.shape[0]
    tiles = cols // 128
    for k in range(maps):
        part = jnp.dot(
            factor_rows[:, k * rank : (k + 1) * rank], moment_ref[k], preferred_element_type=F32
        )
        part = part * scale_ref[k]
        for j in range(tiles):
            rows_ref[pl.ds(maps * j + k, count, stride=maps * tiles), :] = part[
                :, j * 128 : (j + 1) * 128
            ]


def update_kernel(
    core_ref,
    scale_ref,
    own_ref,
    mine_ref,
    other_ref,
    moment_mine_ref,
    moment_other_ref,
    weight_ref,
    step_ref,
    copy_ref,
    factor_ref,
    moment_ref,
    rows_ref,
):
    low = core_ref[0] == 0

    @pl.when(pl.program_id(0) == 0)
    def _():
        mine = moment_mine_ref[...].astype(F32)
        other = moment_other_ref[...].astype(F32)
        first, second = separated(jnp.where(low, mine, other), jnp.where(low, other, mine))
        moment_ref[0] = first.astype(BF16)
        moment_ref[1] = second.astype(BF16)
        low_rank_rows(scale_ref, own_ref[...], moment_ref, step_ref)

    fill_rows(low, mine_ref, other_ref, factor_ref)
    low_rank_rows(scale_ref, factor_ref[...], moment_ref, rows_ref)
    copy_ref[...] = (weight_ref[...].astype(F32) - rows_ref[...]).astype(BF16)


def update(
    core, rate, own_factors, mine, other, moments_mine, moments_other, whole_weights, steps=2
):
    xs, zs, rows, width = mine.shape
    rank, cols = moments_mine.shape
    maps = width // rank
    each = maps * cols // 128
    depth = 2 * xs * rows * zs
    span = depth // steps
    own_depth = own_factors.shape[0]
    block = pl.BlockSpec((xs, zs // steps, rows, width), lambda i: (0, i, 0, 0))
    moment_block = pl.BlockSpec((rank, cols), lambda i: (0, 0))
    return pl.pallas_call(
        update_kernel,
        grid=(steps,),
        in_specs=[
            pl.BlockSpec(memory_space=pltpu.SMEM),
            pl.BlockSpec(memory_space=pltpu.SMEM),
            pl.BlockSpec((own_depth, width), lambda i: (0, 0)),
            block,
            block,
            moment_block,
            moment_block,
            pl.BlockSpec((span * each, 128), lambda i: (i, 0)),
        ],
        out_specs=[
            pl.BlockSpec((own_depth * each, 128), lambda i: (0, 0)),
            pl.BlockSpec((span * each, 128), lambda i: (i, 0)),
        ],
        out_shape=[
            jax.ShapeDtypeStruct((own_depth * each, 128), F32),
            jax.ShapeDtypeStruct((depth * each, 128), BF16),
        ],
        scratch_shapes=[
            pltpu.VMEM((span, width), BF16),
            pltpu.VMEM((maps, rank, cols), BF16),
            pltpu.VMEM((span * each, 128), F32),
        ],
        cost_estimate=pl.CostEstimate(
            flops=2 * depth * width * cols,
            transcendentals=0,
            bytes_accessed=2 * depth * width + 4 * depth * maps * cols,
        ),
        name="low_rank_update",
    )(core, rate, own_factors, mine, other, moments_mine, moments_other, whole_weights)


def as_rows(array):
    depth, maps, cols = array.shape
    tiles = array.reshape(depth, maps, cols // 128, 128).transpose(0, 2, 1, 3)
    return tiles.reshape(depth * maps * cols // 128, 128)


def from_rows(rows, maps, cols):
    tiles = rows.reshape(-1, cols // 128, maps, 128).transpose(0, 2, 1, 3)
    return tiles.reshape(-1, maps, cols)


def sent_to_all(shard, axis):
    copies = jnp.broadcast_to(shard, (lax.axis_size(axis), *shard.shape))
    return lax.all_to_all(copies, axis, split_axis=0, concat_axis=0, tiled=True)


def per_device(
    inputs, queries, keys, values, head_cot, mixing, head_gain, factors, moments, weights
):
    length = inputs.shape[0]
    planes = lax.axis_size(PLANE)
    fs_count = lax.axis_size(FS)
    token_factor = (length * fs_count) ** (-0.5)
    rank_here, maps, cols = moments.shape
    rank = rank_here * fs_count
    core = lax.axis_index(CORE).reshape(1)
    own_factors = factors.reshape(-1, maps * rank)
    whole_weights = lax.all_gather(as_rows(weights).astype(BF16), FS, axis=0, tiled=True)
    columns = sent_to_all(own_factors, DEEP)
    mine = sent_to_all(columns, WIDE)
    d_query, d_value = attention_grads(queries, keys, values, head_cot, mixing, head_gain)
    mine, d_query, d_value = lax.optimization_barrier((mine, d_query, d_value))
    other = lax.ppermute(mine, CORE, SWAP)
    keep, send = project(token_factor, core, mine, other, inputs, d_query, d_value)
    summed = (keep + lax.ppermute(send, CORE, SWAP)).astype(BF16)
    summed = summed.reshape(planes, maps * rank_here, cols)
    parts = lax.all_to_all(summed, PLANE, 0, 0, tiled=True)
    projected = jnp.sum(parts.astype(F32), axis=0).reshape(maps, rank_here, cols)
    new_moments = BETA * moments + projected.transpose(1, 0, 2)
    sent = new_moments.astype(BF16).transpose(1, 0, 2).reshape(maps * rank_here, cols)
    moments_mine = sent_to_all(sent, PLANE)
    moments_other = lax.ppermute(moments_mine, CORE, SWAP)
    squares = moments_mine.astype(F32) ** 2 + moments_other.astype(F32) ** 2
    squares = jnp.sum(squares.reshape(planes, maps, rank_here, cols), axis=(0, 2, 3))
    groups = lax.axis_size("tp")
    totals = squares
    for distance in range(1, groups):
        turn = [(i, (i + distance) % groups) for i in range(groups)]
        totals = totals + lax.ppermute(squares, "tp", turn)
    rate = RATE_BASE / jnp.sqrt(1.0 + totals / (rank * cols * groups))
    step, copies = update(
        core,
        rate,
        own_factors,
        mine,
        other,
        moments_mine.reshape(rank, cols),
        moments_other.reshape(rank, cols),
        whole_weights,
    )
    return (from_rows(step, maps, cols), new_moments, from_rows(copies, maps, cols))


def solution(mesh):
    torus = Mesh(mesh.devices.reshape(8, 4, 2, mesh.shape["tp"]), (*FS, "tp"))
    placed = (
        P(FS, None),
        P(FS, "tp"),
        P(FS, "tp"),
        P(FS, "tp"),
        P(FS, "tp"),
        P("tp"),
        P(),
        P(FS, None, None),
        P(FS, None, "tp"),
        P(FS, None, "tp"),
    )
    return jax.shard_map(
        per_device,
        mesh=torus,
        in_specs=placed,
        out_specs=(P(FS, None, "tp"), P(FS, None, "tp"), P(None, None, "tp")),
        check_vma=False,
    )
```

```python
import functools

import jax
import jax.numpy as jnp
from jax import lax
from jax.experimental import pallas as pl
from jax.experimental.pallas import tpu as pltpu
from jax.sharding import Mesh
from jax.sharding import PartitionSpec as P

PLANE, CORE = ("fs_0", "fs_1"), "fs_2"
FS = (*PLANE, CORE)


EPS = 0.05
BETA = 0.9
RATE_BASE = 0.5
BF16 = jnp.bfloat16
F32 = jnp.float32


def nt_dot(left, right):
    return lax.dot_general(left, right, (((1,), (1,)), ((), ())), preferred_element_type=F32)


def tn_dot(left, right):
    return lax.dot_general(left, right, (((0,), (0,)), ((), ())), preferred_element_type=F32)


def attention_kernel(rows, mix_ref, q_ref, k_ref, v_ref, up_ref, gain_ref, dq_ref, dv_ref, sum_ref):
    length, width = q_ref.shape
    head_dim = width // 2
    factor = head_dim**-0.5
    weight_mix = mix_ref[pl.program_id(0)]
    gain = gain_ref[...]
    for start in range(0, length, rows):
        seen = start + rows
        query = q_ref[start:seen, :]
        keys = k_ref[:seen, :]
        value = v_ref[:seen, :]
        place = lax.broadcasted_iota(jnp.int32, (rows, seen), 0) + start
        causal = lax.broadcasted_iota(jnp.int32, (rows, seen), 1) <= place

        def probs(which):
            cols = slice(which * head_dim, (which + 1) * head_dim)
            scores = nt_dot(query[:, cols], keys[:, cols]) * factor
            scores = jnp.where(causal, scores, -jnp.inf)
            expo = jnp.exp(scores - jnp.max(scores, axis=-1, keepdims=True))
            return expo * (1.0 / jnp.sum(expo, axis=-1, keepdims=True))

        first = probs(0)
        second = weight_mix * probs(1)
        mixed = (first - second).astype(BF16)
        output = jnp.dot(mixed, value, preferred_element_type=F32)
        inverse = lax.rsqrt(jnp.mean(output * output, axis=-1, keepdims=True) + EPS)
        scaled = gain * up_ref[start:seen, :].astype(F32)
        along = jnp.mean(output * scaled, axis=-1, keepdims=True)
        d_out = (inverse * scaled - output * (inverse * inverse * inverse * along)).astype(BF16)
        d_value = tn_dot(mixed, d_out)
        if start:
            sum_ref[:start, :] += d_value[:start]
        sum_ref[start:seen, :] = d_value[start:]
        d_mix = nt_dot(d_out, value)
        first_mix = jnp.sum(first * d_mix, axis=-1, keepdims=True)
        second_mix = jnp.sum(second * d_mix, axis=-1, keepdims=True) * (1.0 / weight_mix)
        d_first = (first * (d_mix - first_mix)).astype(BF16)
        d_second = (second * (second_mix - d_mix)).astype(BF16)
        dq_ref[start:seen, :head_dim] = (
            jnp.dot(d_first, keys[:, :head_dim], preferred_element_type=F32) * factor
        ).astype(BF16)
        dq_ref[start:seen, head_dim:] = (
            jnp.dot(d_second, keys[:, head_dim:], preferred_element_type=F32) * factor
        ).astype(BF16)
    dv_ref[...] = sum_ref[...].astype(BF16)


def attention_grads(queries, keys, values, head_cot, mixing, head_gain, rows=384):
    length, cols = queries.shape
    heads = mixing.shape[0]
    width = cols // heads
    block = pl.BlockSpec((length, width), lambda h: (0, h))
    return pl.pallas_call(
        functools.partial(attention_kernel, rows),
        grid=(heads,),
        in_specs=[
            pl.BlockSpec(memory_space=pltpu.SMEM),
            block,
            block,
            block,
            block,
            pl.BlockSpec((1, width), lambda h: (0, 0)),
        ],
        out_specs=[block, block],
        out_shape=[jax.ShapeDtypeStruct((length, cols), BF16)] * 2,
        scratch_shapes=[pltpu.VMEM((length, width), F32)],
        cost_estimate=pl.CostEstimate(
            flops=20 * length * length * cols,
            transcendentals=2 * heads * length * length,
            bytes_accessed=12 * length * cols,
        ),
        name="attention_grads",
    )(mixing, queries, keys, values, head_cot, head_gain.reshape(1, width))


def interleaved(first, second):
    half = lax.broadcasted_iota(jnp.int32, first.shape, 0) % 8 < 4
    count = first.shape[0]
    even = jnp.where(half, first, pltpu.roll(second, 4, 0))
    odd = jnp.where(half, pltpu.roll(first, count - 4, 0), second)
    return even, odd


def separated(even, odd):
    half = lax.broadcasted_iota(jnp.int32, even.shape, 0) % 8 < 4
    count = even.shape[0]
    first = jnp.where(half, even, pltpu.roll(odd, 4, 0))
    second = jnp.where(half, pltpu.roll(even, count - 4, 0), odd)
    return first, second


def reduce_kernel(core_ref, mine_ref, other_ref, in_ref, rows_ref, red_ref, sum_ref):
    step = pl.program_id(0)
    low = core_ref[0] == 0
    planes, rows, _ = mine_ref.shape
    for plane in range(planes):
        mine, other = mine_ref[plane], other_ref[plane]
        at = 2 * rows * plane
        rows_ref[at : at + rows, :] = jnp.where(low, mine, other)
        rows_ref[at + rows : at + 2 * rows, :] = jnp.where(low, other, mine)
    part = jnp.dot(in_ref[...], rows_ref[...], preferred_element_type=F32)

    @pl.when(step == 0)
    def _():
        sum_ref[...] = part

    @pl.when(step > 0)
    def _():
        sum_ref[...] += part

    @pl.when(step == pl.num_programs(0) - 1)
    def _():
        red_ref[...] = sum_ref[...].astype(BF16)


def reduce_inputs(core, mine, other, inputs, steps=2):
    planes, rows, width = mine.shape
    length, depth = inputs.shape
    block = pl.BlockSpec((planes // steps, rows, width), lambda i: (i, 0, 0))
    return pl.pallas_call(
        reduce_kernel,
        grid=(steps,),
        in_specs=[
            pl.BlockSpec(memory_space=pltpu.SMEM),
            block,
            block,
            pl.BlockSpec((length, depth // steps), lambda i: (0, i)),
        ],
        out_specs=[
            pl.BlockSpec((depth // steps, width), lambda i: (i, 0)),
            pl.BlockSpec((length, width), lambda i: (0, 0)),
        ],
        out_shape=[
            jax.ShapeDtypeStruct((depth, width), BF16),
            jax.ShapeDtypeStruct((length, width), BF16),
        ],
        scratch_shapes=[pltpu.VMEM((length, width), F32)],
        cost_estimate=pl.CostEstimate(
            flops=2 * length * width * depth,
            transcendentals=0,
            bytes_accessed=2 * depth * (length + 2 * width) + 2 * length * width,
        ),
        compiler_params=pltpu.CompilerParams(vmem_limit_bytes=32 << 20),
        name="reduce_inputs",
    )(core, mine, other, inputs)


def project_kernel(scale, core_ref, red_ref, dq_ref, dv_ref, keep_ref, send_ref):
    low = core_ref[0] == 0
    parts = red_ref.shape[0] // 2
    sums = []
    for k, cot_ref in enumerate((dq_ref, dv_ref)):
        reduced = jnp.concatenate([red_ref[k * parts + n] for n in range(parts)], axis=1)
        sums.append(tn_dot(reduced, cot_ref[...]) * scale)
    even, odd = interleaved(*sums)
    keep_ref[...] = jnp.where(low, even, odd)
    send_ref[...] = jnp.where(low, odd, even)


def project(scale, core, reduced, d_query, d_value):
    parts, length, width = reduced.shape
    cols = d_query.shape[1]
    rank = parts * width // 2
    whole = pl.BlockSpec((length, cols), lambda i: (0, 0))
    result = pl.BlockSpec((rank, cols), lambda i: (0, 0))
    return pl.pallas_call(
        functools.partial(project_kernel, scale),
        grid=(1,),
        in_specs=[
            pl.BlockSpec(memory_space=pltpu.SMEM),
            pl.BlockSpec((parts, length, width), lambda i: (0, 0, 0)),
            whole,
            whole,
        ],
        out_specs=[result, result],
        out_shape=[jax.ShapeDtypeStruct((rank, cols), F32)] * 2,
        cost_estimate=pl.CostEstimate(
            flops=4 * length * rank * cols,
            transcendentals=0,
            bytes_accessed=8 * length * cols + 8 * rank * cols,
        ),
        compiler_params=pltpu.CompilerParams(vmem_limit_bytes=32 << 20),
        name="project",
    )(core, reduced, d_query, d_value)


def low_rank_rows(scale_ref, factor_rows, moment_ref, rows_ref):
    maps, rank, cols = moment_ref.shape
    count = factor_rows.shape[0]
    tiles = cols // 128
    for k in range(maps):
        part = jnp.dot(
            factor_rows[:, k * rank : (k + 1) * rank], moment_ref[k], preferred_element_type=F32
        )
        part = part * scale_ref[k]
        for j in range(tiles):
            rows_ref[pl.ds(maps * j + k, count, stride=maps * tiles), :] = part[
                :, j * 128 : (j + 1) * 128
            ]


def update_kernel(place_ref, scale_ref, own_ref, *refs):
    *piece_refs, moment_mine_ref, moment_other_ref, weight_ref = refs[:-5]
    step_ref, copy_ref, factor_ref, moment_ref, rows_ref = refs[-5:]
    low = place_ref[0] == 0
    groups = len(piece_refs)

    @pl.when(pl.program_id(0) == 0)
    def _():
        mine = moment_mine_ref[...].astype(F32)
        other = moment_other_ref[...].astype(F32)
        first, second = separated(jnp.where(low, mine, other), jnp.where(low, other, mine))
        moment_ref[0] = first.astype(BF16)
        moment_ref[1] = second.astype(BF16)
        low_rank_rows(scale_ref, own_ref[...], moment_ref, step_ref)

    for distance, piece_ref in enumerate(piece_refs):
        width = piece_ref.shape[1]
        at = lax.rem(place_ref[1] + (groups - distance), groups) * width
        factor_ref[:, pl.ds(pl.multiple_of(at, width), width)] = piece_ref[...]
    low_rank_rows(scale_ref, factor_ref[...], moment_ref, rows_ref)
    copy_ref[...] = (weight_ref[...].astype(F32) - rows_ref[...]).astype(BF16)


def update(place, rate, own_factors, pieces, moments_mine, moments_other, whole_weights, steps=2):
    depth, part = pieces[0].shape
    own_depth, width = own_factors.shape
    rank, cols = moments_mine.shape
    maps = width // rank
    each = maps * cols // 128
    span = depth // steps
    moment_block = pl.BlockSpec((rank, cols), lambda i: (0, 0))
    row_block = pl.BlockSpec((span * each, 128), lambda i: (i, 0))
    return pl.pallas_call(
        update_kernel,
        grid=(steps,),
        in_specs=[
            pl.BlockSpec(memory_space=pltpu.SMEM),
            pl.BlockSpec(memory_space=pltpu.SMEM),
            pl.BlockSpec((own_depth, width), lambda i: (0, 0)),
            *[pl.BlockSpec((span, part), lambda i: (i, 0))] * len(pieces),
            moment_block,
            moment_block,
            row_block,
        ],
        out_specs=[pl.BlockSpec((own_depth * each, 128), lambda i: (0, 0)), row_block],
        out_shape=[
            jax.ShapeDtypeStruct((own_depth * each, 128), F32),
            jax.ShapeDtypeStruct((depth * each, 128), BF16),
        ],
        scratch_shapes=[
            pltpu.VMEM((span, width), BF16),
            pltpu.VMEM((maps, rank, cols), BF16),
            pltpu.VMEM((span * each, 128), F32),
        ],
        cost_estimate=pl.CostEstimate(
            flops=2 * depth * width * cols,
            transcendentals=0,
            bytes_accessed=2 * depth * width + 4 * depth * maps * cols,
        ),
        name="low_rank_update",
    )(place, rate, own_factors, *pieces, moments_mine, moments_other, whole_weights)


def as_rows(array):
    depth, maps, cols = array.shape
    tiles = array.reshape(depth, maps, cols // 128, 128).transpose(0, 2, 1, 3)
    return tiles.reshape(depth * maps * cols // 128, 128)


def from_rows(rows, maps, cols):
    tiles = rows.reshape(-1, cols // 128, maps, 128).transpose(0, 2, 1, 3)
    return tiles.reshape(-1, maps, cols)


def sent_to_all(shard, axis):
    copies = jnp.broadcast_to(shard, (lax.axis_size(axis), *shard.shape))
    return lax.all_to_all(copies, axis, split_axis=0, concat_axis=0, tiled=True)


def turned(array, axis, distance):
    count = lax.axis_size(axis)
    return lax.ppermute(array, axis, [(i, (i + distance) % count) for i in range(count)])


def per_device(
    inputs, queries, keys, values, head_cot, mixing, head_gain, factors, moments, weights
):
    length = inputs.shape[0]
    planes = lax.axis_size(PLANE)
    fs_count = lax.axis_size(FS)
    groups = lax.axis_size("tp")
    token_factor = (length * fs_count) ** (-0.5)
    rank_here, maps, cols = moments.shape
    rank = rank_here * fs_count
    width = maps * rank
    place = jnp.stack([lax.axis_index(CORE), lax.axis_index("tp")])
    weight_rows = lax.optimization_barrier(as_rows(weights))
    whole_weights = lax.all_gather(weight_rows.astype(BF16), FS, axis=0, tiled=True)
    own_factors = factors.reshape(-1, width)
    part = width // groups
    own_part = lax.dynamic_slice_in_dim(own_factors, lax.axis_index("tp") * part, part, 1)
    mine = sent_to_all(own_part, PLANE)
    d_query, d_value = attention_grads(queries, keys, values, head_cot, mixing, head_gain)
    mine, d_query, d_value = lax.optimization_barrier((mine, d_query, d_value))
    other = turned(mine, CORE, 1)
    columns, reduced = reduce_inputs(place, mine, other, inputs)
    reduced, columns = lax.optimization_barrier((sent_to_all(reduced, "tp"), columns))
    pieces = [columns] + [turned(columns, "tp", n) for n in range(1, groups)]
    keep, send = project(token_factor, place, reduced, d_query, d_value)
    summed = (keep + turned(send, CORE, 1)).astype(BF16)
    summed = summed.reshape(planes, maps * rank_here, cols)
    parts = lax.all_to_all(summed, PLANE, 0, 0, tiled=True)
    projected = jnp.sum(parts.astype(F32), axis=0).reshape(maps, rank_here, cols)
    new_moments = BETA * moments + projected.transpose(1, 0, 2)
    sent = new_moments.astype(BF16).transpose(1, 0, 2).reshape(maps * rank_here, cols)
    moments_mine, pieces = lax.optimization_barrier((sent_to_all(sent, PLANE), pieces))
    moments_other = turned(moments_mine, CORE, 1)
    squares = moments_mine.astype(F32) ** 2 + moments_other.astype(F32) ** 2
    squares = jnp.sum(squares.reshape(planes, maps, rank_here, cols), axis=(0, 2, 3))
    totals = squares
    for distance in range(1, groups):
        totals = totals + turned(squares, "tp", distance)
    rate = RATE_BASE / jnp.sqrt(1.0 + totals / (rank * cols * groups))
    step, copies = update(
        place,
        rate,
        own_factors,
        pieces,
        moments_mine.reshape(rank, cols),
        moments_other.reshape(rank, cols),
        whole_weights,
    )
    return (from_rows(step, maps, cols), new_moments, from_rows(copies, maps, cols))


def solution(mesh):
    torus = Mesh(mesh.devices.reshape(8, 4, 2, mesh.shape["tp"]), (*FS, "tp"))
    placed = (
        P(FS, None),
        P(FS, "tp"),
        P(FS, "tp"),
        P(FS, "tp"),
        P(FS, "tp"),
        P("tp"),
        P(),
        P(FS, None, None),
        P(FS, None, "tp"),
        P(FS, None, "tp"),
    )
    return jax.shard_map(
        per_device,
        mesh=torus,
        in_specs=placed,
        out_specs=(P(FS, None, "tp"), P(FS, None, "tp"), P(None, None, "tp")),
        check_vma=False,
    )
```

```python
import functools

import jax
import jax.numpy as jnp
from jax import lax
from jax.experimental import pallas as pl
from jax.experimental.pallas import tpu as pltpu
from jax.sharding import Mesh
from jax.sharding import PartitionSpec as P

DEEP, WIDE, CORE = "fs_0", "fs_1", "fs_2"
PLANE = (DEEP, WIDE)
FS = (*PLANE, CORE)


EPS = 0.05
BETA = 0.9
RATE_BASE = 0.5
BF16 = jnp.bfloat16
F32 = jnp.float32


def nt_dot(left, right):
    return lax.dot_general(left, right, (((1,), (1,)), ((), ())), preferred_element_type=F32)


def tn_dot(left, right):
    return lax.dot_general(left, right, (((0,), (0,)), ((), ())), preferred_element_type=F32)


def attention_kernel(rows, mix_ref, q_ref, k_ref, v_ref, up_ref, gain_ref, dq_ref, dv_ref, sum_ref):
    length, width = q_ref.shape
    head_dim = width // 2
    factor = head_dim**-0.5
    weight_mix = mix_ref[pl.program_id(0)]
    gain = gain_ref[...]
    for start in range(0, length, rows):
        seen = start + rows
        query = q_ref[start:seen, :]
        keys = k_ref[:seen, :]
        value = v_ref[:seen, :]
        place = lax.broadcasted_iota(jnp.int32, (rows, seen), 0) + start
        causal = lax.broadcasted_iota(jnp.int32, (rows, seen), 1) <= place

        def probs(which):
            cols = slice(which * head_dim, (which + 1) * head_dim)
            scores = nt_dot(query[:, cols], keys[:, cols]) * factor
            scores = jnp.where(causal, scores, -jnp.inf)
            expo = jnp.exp(scores - jnp.max(scores, axis=-1, keepdims=True))
            return expo * (1.0 / jnp.sum(expo, axis=-1, keepdims=True))

        first = probs(0)
        second = weight_mix * probs(1)
        mixed = (first - second).astype(BF16)
        output = jnp.dot(mixed, value, preferred_element_type=F32)
        inverse = lax.rsqrt(jnp.mean(output * output, axis=-1, keepdims=True) + EPS)
        scaled = gain * up_ref[start:seen, :].astype(F32)
        along = jnp.mean(output * scaled, axis=-1, keepdims=True)
        d_out = (inverse * scaled - output * (inverse * inverse * inverse * along)).astype(BF16)
        d_value = tn_dot(mixed, d_out)
        if start:
            sum_ref[:start, :] += d_value[:start]
        sum_ref[start:seen, :] = d_value[start:]
        d_mix = nt_dot(d_out, value)
        first_mix = jnp.sum(first * d_mix, axis=-1, keepdims=True)
        second_mix = jnp.sum(second * d_mix, axis=-1, keepdims=True) * (1.0 / weight_mix)
        d_first = (first * (d_mix - first_mix)).astype(BF16)
        d_second = (second * (second_mix - d_mix)).astype(BF16)
        dq_ref[start:seen, :head_dim] = (
            jnp.dot(d_first, keys[:, :head_dim], preferred_element_type=F32) * factor
        ).astype(BF16)
        dq_ref[start:seen, head_dim:] = (
            jnp.dot(d_second, keys[:, head_dim:], preferred_element_type=F32) * factor
        ).astype(BF16)
    dv_ref[...] = sum_ref[...].astype(BF16)


def attention_grads(queries, keys, values, head_cot, mixing, head_gain, rows=384):
    length, cols = queries.shape
    heads = mixing.shape[0]
    width = cols // heads
    block = pl.BlockSpec((length, width), lambda h: (0, h))
    return pl.pallas_call(
        functools.partial(attention_kernel, rows),
        grid=(heads,),
        in_specs=[
            pl.BlockSpec(memory_space=pltpu.SMEM),
            block,
            block,
            block,
            block,
            pl.BlockSpec((1, width), lambda h: (0, 0)),
        ],
        out_specs=[block, block],
        out_shape=[jax.ShapeDtypeStruct((length, cols), BF16)] * 2,
        scratch_shapes=[pltpu.VMEM((length, width), F32)],
        cost_estimate=pl.CostEstimate(
            flops=20 * length * length * cols,
            transcendentals=2 * heads * length * length,
            bytes_accessed=12 * length * cols,
        ),
        name="attention_grads",
    )(mixing, queries, keys, values, head_cot, head_gain.reshape(1, width))


def interleaved(first, second):
    half = lax.broadcasted_iota(jnp.int32, first.shape, 0) % 8 < 4
    count = first.shape[0]
    even = jnp.where(half, first, pltpu.roll(second, 4, 0))
    odd = jnp.where(half, pltpu.roll(first, count - 4, 0), second)
    return even, odd


def separated(even, odd):
    half = lax.broadcasted_iota(jnp.int32, even.shape, 0) % 8 < 4
    count = even.shape[0]
    first = jnp.where(half, even, pltpu.roll(odd, 4, 0))
    second = jnp.where(half, pltpu.roll(even, count - 4, 0), odd)
    return first, second


def reduce_kernel(core_ref, mine_ref, other_ref, in_ref, rows_ref, red_ref, sum_ref):
    step = pl.program_id(0)
    low = core_ref[0] == 0
    planes, rows, _ = mine_ref.shape
    for plane in range(planes):
        mine, other = mine_ref[plane], other_ref[plane]
        at = 2 * rows * plane
        rows_ref[at : at + rows, :] = jnp.where(low, mine, other)
        rows_ref[at + rows : at + 2 * rows, :] = jnp.where(low, other, mine)
    part = jnp.dot(in_ref[...], rows_ref[...], preferred_element_type=F32)

    @pl.when(step == 0)
    def _():
        sum_ref[...] = part

    @pl.when(step > 0)
    def _():
        sum_ref[...] += part

    @pl.when(step == pl.num_programs(0) - 1)
    def _():
        red_ref[...] = sum_ref[...].astype(BF16)


def reduce_inputs(core, mine, other, inputs, steps=2):
    planes, rows, width = mine.shape
    length, depth = inputs.shape
    block = pl.BlockSpec((planes // steps, rows, width), lambda i: (i, 0, 0))
    return pl.pallas_call(
        reduce_kernel,
        grid=(steps,),
        in_specs=[
            pl.BlockSpec(memory_space=pltpu.SMEM),
            block,
            block,
            pl.BlockSpec((length, depth // steps), lambda i: (0, i)),
        ],
        out_specs=[
            pl.BlockSpec((depth // steps, width), lambda i: (i, 0)),
            pl.BlockSpec((length, width), lambda i: (0, 0)),
        ],
        out_shape=[
            jax.ShapeDtypeStruct((depth, width), BF16),
            jax.ShapeDtypeStruct((length, width), BF16),
        ],
        scratch_shapes=[pltpu.VMEM((length, width), F32)],
        cost_estimate=pl.CostEstimate(
            flops=2 * length * width * depth,
            transcendentals=0,
            bytes_accessed=2 * depth * (length + 2 * width) + 2 * length * width,
        ),
        compiler_params=pltpu.CompilerParams(vmem_limit_bytes=32 << 20),
        name="reduce_inputs",
    )(core, mine, other, inputs)


def project_kernel(scale, core_ref, red_ref, dq_ref, dv_ref, keep_ref, send_ref):
    low = core_ref[0] == 0
    parts = red_ref.shape[0] // 2
    sums = []
    for k, cot_ref in enumerate((dq_ref, dv_ref)):
        reduced = jnp.concatenate([red_ref[k * parts + n] for n in range(parts)], axis=1)
        sums.append(tn_dot(reduced, cot_ref[...]) * scale)
    even, odd = interleaved(*sums)
    keep_ref[...] = jnp.where(low, even, odd)
    send_ref[...] = jnp.where(low, odd, even)


def project(scale, core, reduced, d_query, d_value):
    parts, length, width = reduced.shape
    cols = d_query.shape[1]
    rank = parts * width // 2
    whole = pl.BlockSpec((length, cols), lambda i: (0, 0))
    result = pl.BlockSpec((rank, cols), lambda i: (0, 0))
    return pl.pallas_call(
        functools.partial(project_kernel, scale),
        grid=(1,),
        in_specs=[
            pl.BlockSpec(memory_space=pltpu.SMEM),
            pl.BlockSpec((parts, length, width), lambda i: (0, 0, 0)),
            whole,
            whole,
        ],
        out_specs=[result, result],
        out_shape=[jax.ShapeDtypeStruct((rank, cols), F32)] * 2,
        cost_estimate=pl.CostEstimate(
            flops=4 * length * rank * cols,
            transcendentals=0,
            bytes_accessed=8 * length * cols + 8 * rank * cols,
        ),
        name="project",
    )(core, reduced, d_query, d_value)


def low_rank_rows(scale_ref, factor_rows, moment_ref, rows_ref):
    maps, rank, cols = moment_ref.shape
    count = factor_rows.shape[0]
    tiles = cols // 128
    for k in range(maps):
        part = jnp.dot(
            factor_rows[:, k * rank : (k + 1) * rank], moment_ref[k], preferred_element_type=F32
        )
        part = part * scale_ref[k]
        for j in range(tiles):
            rows_ref[pl.ds(maps * j + k, count, stride=maps * tiles), :] = part[
                :, j * 128 : (j + 1) * 128
            ]


def update_kernel(groups, place_ref, scale_ref, own_ref, *refs):
    moment_mine_ref, moment_other_ref = refs[:2]
    piece_refs, weight_refs = refs[2 : 2 + groups], refs[2 + groups : -5]
    step_ref, copy_ref, factor_ref, moment_ref, rows_ref = refs[-5:]
    low = place_ref[0] == 0

    @pl.when(pl.program_id(0) == 0)
    def _():
        mine = moment_mine_ref[...].astype(F32)
        other = moment_other_ref[...].astype(F32)
        first, second = separated(jnp.where(low, mine, other), jnp.where(low, other, mine))
        moment_ref[0] = first.astype(BF16)
        moment_ref[1] = second.astype(BF16)
        low_rank_rows(scale_ref, own_ref[...], moment_ref, step_ref)

    for distance, piece_ref in enumerate(piece_refs):
        width = piece_ref.shape[1]
        at = lax.rem(place_ref[1] + (groups - distance), groups) * width
        factor_ref[:, pl.ds(pl.multiple_of(at, width), width)] = piece_ref[...]
    low_rank_rows(scale_ref, factor_ref[...], moment_ref, rows_ref)
    wide = len(weight_refs) // 2
    all_zs, count, _ = weight_refs[0].shape
    zs = copy_ref.shape[0] // (2 * wide * count)
    for distance in range(wide):
        mine_ref, other_ref = weight_refs[2 * distance : 2 * distance + 2]
        x = lax.rem(place_ref[2] + (wide - distance), wide)
        for z in range(zs):
            ahead = lax.rem(pl.program_id(0) * zs + z + all_zs - place_ref[3], all_zs)
            slot = 4 * lax.rem(ahead, 2) + 2 * lax.rem(ahead // 2, 2) + ahead // 4
            halves = mine_ref[slot], other_ref[slot]
            for owner in range(2):
                weight = jnp.where(low, halves[owner], halves[1 - owner])
                at = pl.multiple_of(count * (2 * (z * wide + x) + owner), count)
                part = pl.ds(at, count)
                copy_ref[part, :] = (weight.astype(F32) - rows_ref[part, :]).astype(BF16)


def update(place, rate, own_factors, moments_mine, moments_other, pieces, weight_pieces, steps=2):
    depth, part = pieces[0].shape
    own_depth, width = own_factors.shape
    rank, cols = moments_mine.shape
    maps = width // rank
    each = maps * cols // 128
    span = depth // steps
    moment_block = pl.BlockSpec((rank, cols), lambda i: (0, 0))
    row_block = pl.BlockSpec((span * each, 128), lambda i: (i, 0))
    weight_block = pl.BlockSpec(weight_pieces[0].shape, lambda i: (0, 0, 0))
    return pl.pallas_call(
        functools.partial(update_kernel, len(pieces)),
        grid=(steps,),
        in_specs=[
            pl.BlockSpec(memory_space=pltpu.SMEM),
            pl.BlockSpec(memory_space=pltpu.SMEM),
            pl.BlockSpec((own_depth, width), lambda i: (0, 0)),
            moment_block,
            moment_block,
            *[pl.BlockSpec((span, part), lambda i: (i, 0))] * len(pieces),
            *[weight_block] * len(weight_pieces),
        ],
        out_specs=[pl.BlockSpec((own_depth * each, 128), lambda i: (0, 0)), row_block],
        out_shape=[
            jax.ShapeDtypeStruct((own_depth * each, 128), F32),
            jax.ShapeDtypeStruct((depth * each, 128), BF16),
        ],
        scratch_shapes=[
            pltpu.VMEM((span, width), BF16),
            pltpu.VMEM((maps, rank, cols), BF16),
            pltpu.VMEM((span * each, 128), F32),
        ],
        cost_estimate=pl.CostEstimate(
            flops=2 * depth * width * cols,
            transcendentals=0,
            bytes_accessed=2 * depth * width + 4 * depth * maps * cols,
        ),
        compiler_params=pltpu.CompilerParams(vmem_limit_bytes=40 << 20),
        name="low_rank_update",
    )(place, rate, own_factors, moments_mine, moments_other, *pieces, *weight_pieces)


def as_rows(array):
    depth, maps, cols = array.shape
    tiles = array.reshape(depth, maps, cols // 128, 128).transpose(0, 2, 1, 3)
    return tiles.reshape(depth * maps * cols // 128, 128)


def from_rows(rows, maps, cols):
    tiles = rows.reshape(-1, cols // 128, maps, 128).transpose(0, 2, 1, 3)
    return tiles.reshape(-1, maps, cols)


def sent_to_all(shard, axis):
    copies = jnp.broadcast_to(shard, (lax.axis_size(axis), *shard.shape))
    return lax.all_to_all(copies, axis, split_axis=0, concat_axis=0, tiled=True)


def turned(array, axis, distance):
    count = lax.axis_size(axis)
    return lax.ppermute(array, axis, [(i, (i + distance) % count) for i in range(count)])


def per_device(
    inputs, queries, keys, values, head_cot, mixing, head_gain, factors, moments, weights
):
    length = inputs.shape[0]
    planes = lax.axis_size(PLANE)
    fs_count = lax.axis_size(FS)
    groups = lax.axis_size("tp")
    token_factor = (length * fs_count) ** (-0.5)
    rank_here, maps, cols = moments.shape
    rank = rank_here * fs_count
    width = maps * rank
    place = jnp.stack([lax.axis_index(axis) for axis in (CORE, "tp", WIDE, DEEP)])
    own_factors = factors.reshape(-1, width)
    part = width // groups
    own_part = lax.dynamic_slice_in_dim(own_factors, lax.axis_index("tp") * part, part, 1)
    mine = sent_to_all(own_part, PLANE)
    weight_rows = lax.optimization_barrier(as_rows(weights)).astype(BF16)[None]
    weight_columns = lax.optimization_barrier((weight_rows, turned(weight_rows, DEEP, -4)))
    d_query, d_value = attention_grads(queries, keys, values, head_cot, mixing, head_gain)
    mine, d_query, d_value, weight_columns = lax.optimization_barrier(
        (mine, d_query, d_value, jnp.concatenate(weight_columns))
    )
    weight_columns = jnp.concatenate([weight_columns, turned(weight_columns, DEEP, -2)])
    other = turned(mine, CORE, 1)
    columns, reduced = reduce_inputs(place, mine, other, inputs)
    reduced, weight_columns = lax.optimization_barrier((reduced, weight_columns))
    weight_columns = jnp.concatenate([weight_columns, turned(weight_columns, DEEP, -1)])
    reduced, columns, weight_columns = lax.optimization_barrier(
        (sent_to_all(reduced, "tp"), columns, weight_columns)
    )
    pieces = [columns] + [turned(columns, "tp", n) for n in range(1, groups)]
    keep, send = project(token_factor, place, reduced, d_query, d_value)
    summed = (keep + turned(send, CORE, 1)).astype(BF16)
    summed = summed.reshape(planes, maps * rank_here, cols)
    summed, weight_columns = lax.optimization_barrier((summed, weight_columns))
    before = turned(weight_columns, WIDE, 1)
    after = turned(weight_columns, WIDE, -1)
    parts = lax.all_to_all(summed, PLANE, 0, 0, tiled=True)
    projected = jnp.sum(parts.astype(F32), axis=0).reshape(maps, rank_here, cols)
    new_moments = BETA * moments + projected.transpose(1, 0, 2)
    sent = new_moments.astype(BF16).transpose(1, 0, 2).reshape(maps * rank_here, cols)
    sent, before, after = lax.optimization_barrier((sent, before, after))
    half = before.shape[0] // 2
    across = [turned(before[:half], WIDE, 1), turned(after[half:], WIDE, -1)]
    weight_pieces = [weight_columns, before, jnp.concatenate(across), after]
    weight_pieces = [piece for mine in weight_pieces for piece in (mine, turned(mine, CORE, 1))]
    moments_mine, pieces = lax.optimization_barrier((sent_to_all(sent, PLANE), pieces))
    moments_other = turned(moments_mine, CORE, 1)
    squares = moments_mine.astype(F32) ** 2 + moments_other.astype(F32) ** 2
    squares = jnp.sum(squares.reshape(planes, maps, rank_here, cols), axis=(0, 2, 3))
    totals = squares
    for distance in range(1, groups):
        totals = totals + turned(squares, "tp", distance)
    rate = RATE_BASE / jnp.sqrt(1.0 + totals / (rank * cols * groups))
    step, copies = update(
        place,
        rate,
        own_factors,
        moments_mine.reshape(rank, cols),
        moments_other.reshape(rank, cols),
        pieces,
        weight_pieces,
    )
    return (from_rows(step, maps, cols), new_moments, from_rows(copies, maps, cols))


def solution(mesh):
    torus = Mesh(mesh.devices.reshape(8, 4, 2, mesh.shape["tp"]), (*FS, "tp"))
    placed = (
        P(FS, None),
        P(FS, "tp"),
        P(FS, "tp"),
        P(FS, "tp"),
        P(FS, "tp"),
        P("tp"),
        P(),
        P(FS, None, None),
        P(FS, None, "tp"),
        P(FS, None, "tp"),
    )
    return jax.shard_map(
        per_device,
        mesh=torus,
        in_specs=placed,
        out_specs=(P(FS, None, "tp"), P(FS, None, "tp"), P(None, None, "tp")),
        check_vma=False,
    )
```

```python
import functools

import jax
import jax.numpy as jnp
from jax import lax
from jax.experimental import pallas as pl
from jax.experimental.pallas import tpu as pltpu
from jax.sharding import Mesh
from jax.sharding import PartitionSpec as P

DEEP, WIDE, CORE = "fs_0", "fs_1", "fs_2"
PLANE = (DEEP, WIDE)
FS = (*PLANE, CORE)


EPS = 0.05
BETA = 0.9
RATE_BASE = 0.5
BF16 = jnp.bfloat16
F32 = jnp.float32


def nt_dot(left, right):
    return lax.dot_general(left, right, (((1,), (1,)), ((), ())), preferred_element_type=F32)


def tn_dot(left, right):
    return lax.dot_general(left, right, (((0,), (0,)), ((), ())), preferred_element_type=F32)


def attention_kernel(rows, mix_ref, q_ref, k_ref, v_ref, up_ref, gain_ref, dq_ref, dv_ref, sum_ref):
    length, width = q_ref.shape
    head_dim = width // 2
    factor = head_dim**-0.5
    weight_mix = mix_ref[pl.program_id(0)]
    gain = gain_ref[...]
    for start in range(0, length, rows):
        seen = start + rows
        query = q_ref[start:seen, :]
        keys = k_ref[:seen, :]
        value = v_ref[:seen, :]
        place = lax.broadcasted_iota(jnp.int32, (rows, seen), 0) + start
        causal = lax.broadcasted_iota(jnp.int32, (rows, seen), 1) <= place

        def probs(which):
            cols = slice(which * head_dim, (which + 1) * head_dim)
            scores = nt_dot(query[:, cols], keys[:, cols]) * factor
            scores = jnp.where(causal, scores, -jnp.inf)
            expo = jnp.exp(scores - jnp.max(scores, axis=-1, keepdims=True))
            return expo * (1.0 / jnp.sum(expo, axis=-1, keepdims=True))

        first = probs(0)
        second = weight_mix * probs(1)
        mixed = (first - second).astype(BF16)
        output = jnp.dot(mixed, value, preferred_element_type=F32)
        inverse = lax.rsqrt(jnp.mean(output * output, axis=-1, keepdims=True) + EPS)
        scaled = gain * up_ref[start:seen, :].astype(F32)
        along = jnp.mean(output * scaled, axis=-1, keepdims=True)
        d_out = (inverse * scaled - output * (inverse * inverse * inverse * along)).astype(BF16)
        d_value = tn_dot(mixed, d_out)
        if start:
            sum_ref[:start, :] += d_value[:start]
        sum_ref[start:seen, :] = d_value[start:]
        d_mix = nt_dot(d_out, value)
        first_mix = jnp.sum(first * d_mix, axis=-1, keepdims=True)
        second_mix = jnp.sum(second * d_mix, axis=-1, keepdims=True) * (1.0 / weight_mix)
        d_first = (first * (d_mix - first_mix)).astype(BF16)
        d_second = (second * (second_mix - d_mix)).astype(BF16)
        dq_ref[start:seen, :head_dim] = (
            jnp.dot(d_first, keys[:, :head_dim], preferred_element_type=F32) * factor
        ).astype(BF16)
        dq_ref[start:seen, head_dim:] = (
            jnp.dot(d_second, keys[:, head_dim:], preferred_element_type=F32) * factor
        ).astype(BF16)
    dv_ref[...] = sum_ref[...].astype(BF16)


def attention_grads(queries, keys, values, head_cot, mixing, head_gain, rows=384):
    length, cols = queries.shape
    heads = mixing.shape[0]
    width = cols // heads
    block = pl.BlockSpec((length, width), lambda h: (0, h))
    return pl.pallas_call(
        functools.partial(attention_kernel, rows),
        grid=(heads,),
        in_specs=[
            pl.BlockSpec(memory_space=pltpu.SMEM),
            block,
            block,
            block,
            block,
            pl.BlockSpec((1, width), lambda h: (0, 0)),
        ],
        out_specs=[block, block],
        out_shape=[jax.ShapeDtypeStruct((length, cols), BF16)] * 2,
        scratch_shapes=[pltpu.VMEM((length, width), F32)],
        cost_estimate=pl.CostEstimate(
            flops=20 * length * length * cols,
            transcendentals=2 * heads * length * length,
            bytes_accessed=12 * length * cols,
        ),
        name="attention_grads",
    )(mixing, queries, keys, values, head_cot, head_gain.reshape(1, width))


def interleaved(first, second):
    half = lax.broadcasted_iota(jnp.int32, first.shape, 0) % 8 < 4
    count = first.shape[0]
    even = jnp.where(half, first, pltpu.roll(second, 4, 0))
    odd = jnp.where(half, pltpu.roll(first, count - 4, 0), second)
    return even, odd


def separated(even, odd):
    half = lax.broadcasted_iota(jnp.int32, even.shape, 0) % 8 < 4
    count = even.shape[0]
    first = jnp.where(half, even, pltpu.roll(odd, 4, 0))
    second = jnp.where(half, pltpu.roll(even, count - 4, 0), odd)
    return first, second


def reduce_kernel(core_ref, mine_ref, other_ref, in_ref, rows_ref, red_ref, sum_ref):
    step = pl.program_id(0)
    low = core_ref[0] == 0
    planes, rows, _ = mine_ref.shape
    for plane in range(planes):
        mine, other = mine_ref[plane], other_ref[plane]
        at = 2 * rows * plane
        rows_ref[at : at + rows, :] = jnp.where(low, mine, other)
        rows_ref[at + rows : at + 2 * rows, :] = jnp.where(low, other, mine)
    part = jnp.dot(in_ref[...], rows_ref[...], preferred_element_type=F32)

    @pl.when(step == 0)
    def _():
        sum_ref[...] = part

    @pl.when(step > 0)
    def _():
        sum_ref[...] += part

    @pl.when(step == pl.num_programs(0) - 1)
    def _():
        red_ref[...] = sum_ref[...].astype(BF16)


def reduce_inputs(core, mine, other, inputs, steps=2):
    planes, rows, width = mine.shape
    length, depth = inputs.shape
    block = pl.BlockSpec((planes // steps, rows, width), lambda i: (i, 0, 0))
    return pl.pallas_call(
        reduce_kernel,
        grid=(steps,),
        in_specs=[
            pl.BlockSpec(memory_space=pltpu.SMEM),
            block,
            block,
            pl.BlockSpec((length, depth // steps), lambda i: (0, i)),
        ],
        out_specs=[
            pl.BlockSpec((depth // steps, width), lambda i: (i, 0)),
            pl.BlockSpec((length, width), lambda i: (0, 0)),
        ],
        out_shape=[
            jax.ShapeDtypeStruct((depth, width), BF16),
            jax.ShapeDtypeStruct((length, width), BF16),
        ],
        scratch_shapes=[pltpu.VMEM((length, width), F32)],
        cost_estimate=pl.CostEstimate(
            flops=2 * length * width * depth,
            transcendentals=0,
            bytes_accessed=2 * depth * (length + 2 * width) + 2 * length * width,
        ),
        compiler_params=pltpu.CompilerParams(vmem_limit_bytes=32 << 20),
        name="reduce_inputs",
    )(core, mine, other, inputs)


def project_kernel(scale, core_ref, red_ref, dq_ref, dv_ref, keep_ref, send_ref):
    low = core_ref[0] == 0
    parts = red_ref.shape[0] // 2
    sums = []
    for k, cot_ref in enumerate((dq_ref, dv_ref)):
        reduced = jnp.concatenate([red_ref[k * parts + n] for n in range(parts)], axis=1)
        sums.append(tn_dot(reduced, cot_ref[...]) * scale)
    even, odd = interleaved(*sums)
    keep_ref[...] = jnp.where(low, even, odd)
    send_ref[...] = jnp.where(low, odd, even)


def project(scale, core, reduced, d_query, d_value):
    parts, length, width = reduced.shape
    cols = d_query.shape[1]
    rank = parts * width // 2
    whole = pl.BlockSpec((length, cols), lambda i: (0, 0))
    result = pl.BlockSpec((rank, cols), lambda i: (0, 0))
    return pl.pallas_call(
        functools.partial(project_kernel, scale),
        grid=(1,),
        in_specs=[
            pl.BlockSpec(memory_space=pltpu.SMEM),
            pl.BlockSpec((parts, length, width), lambda i: (0, 0, 0)),
            whole,
            whole,
        ],
        out_specs=[result, result],
        out_shape=[jax.ShapeDtypeStruct((rank, cols), F32)] * 2,
        cost_estimate=pl.CostEstimate(
            flops=4 * length * rank * cols,
            transcendentals=0,
            bytes_accessed=8 * length * cols + 8 * rank * cols,
        ),
        compiler_params=pltpu.CompilerParams(vmem_limit_bytes=32 << 20),
        name="project",
    )(core, reduced, d_query, d_value)


def low_rank_rows(scale_ref, factor_rows, moment_ref, rows_ref):
    maps, rank, cols = moment_ref.shape
    count = factor_rows.shape[0]
    tiles = cols // 128
    for k in range(maps):
        part = jnp.dot(
            factor_rows[:, k * rank : (k + 1) * rank], moment_ref[k], preferred_element_type=F32
        )
        part = part * scale_ref[k]
        for j in range(tiles):
            rows_ref[pl.ds(maps * j + k, count, stride=maps * tiles), :] = part[
                :, j * 128 : (j + 1) * 128
            ]


def update_kernel(groups, place_ref, scale_ref, own_ref, *refs):
    moment_mine_ref, moment_other_ref = refs[:2]
    piece_refs, weight_refs = refs[2 : 2 + groups], refs[2 + groups : -5]
    step_ref, copy_ref, factor_ref, moment_ref, rows_ref = refs[-5:]
    low = place_ref[0] == 0

    @pl.when(pl.program_id(0) == 0)
    def _():
        mine = moment_mine_ref[...].astype(F32)
        other = moment_other_ref[...].astype(F32)
        first, second = separated(jnp.where(low, mine, other), jnp.where(low, other, mine))
        moment_ref[0] = first.astype(BF16)
        moment_ref[1] = second.astype(BF16)
        low_rank_rows(scale_ref, own_ref[...], moment_ref, step_ref)

    for distance, piece_ref in enumerate(piece_refs):
        width = piece_ref.shape[1]
        at = lax.rem(place_ref[1] + (groups - distance), groups) * width
        factor_ref[:, pl.ds(pl.multiple_of(at, width), width)] = piece_ref[...]
    low_rank_rows(scale_ref, factor_ref[...], moment_ref, rows_ref)
    wide = len(weight_refs) // 2
    all_zs, count, _ = weight_refs[0].shape
    zs = copy_ref.shape[0] // (2 * wide * count)
    for distance in range(wide):
        mine_ref, other_ref = weight_refs[2 * distance : 2 * distance + 2]
        x = lax.rem(place_ref[2] + (wide - distance), wide)
        for z in range(zs):
            ahead = lax.rem(pl.program_id(0) * zs + z + all_zs - place_ref[3], all_zs)
            slot = 4 * lax.rem(ahead, 2) + 2 * lax.rem(ahead // 2, 2) + ahead // 4
            halves = mine_ref[slot], other_ref[slot]
            for owner in range(2):
                weight = jnp.where(low, halves[owner], halves[1 - owner])
                at = pl.multiple_of(count * (2 * (z * wide + x) + owner), count)
                part = pl.ds(at, count)
                copy_ref[part, :] = (weight.astype(F32) - rows_ref[part, :]).astype(BF16)


def update(place, rate, own_factors, moments_mine, moments_other, pieces, weight_pieces, steps=2):
    depth, part = pieces[0].shape
    own_depth, width = own_factors.shape
    rank, cols = moments_mine.shape
    maps = width // rank
    each = maps * cols // 128
    span = depth // steps
    moment_block = pl.BlockSpec((rank, cols), lambda i: (0, 0))
    row_block = pl.BlockSpec((span * each, 128), lambda i: (i, 0))
    weight_block = pl.BlockSpec(weight_pieces[0].shape, lambda i: (0, 0, 0))
    return pl.pallas_call(
        functools.partial(update_kernel, len(pieces)),
        grid=(steps,),
        in_specs=[
            pl.BlockSpec(memory_space=pltpu.SMEM),
            pl.BlockSpec(memory_space=pltpu.SMEM),
            pl.BlockSpec((own_depth, width), lambda i: (0, 0)),
            moment_block,
            moment_block,
            *[pl.BlockSpec((span, part), lambda i: (i, 0))] * len(pieces),
            *[weight_block] * len(weight_pieces),
        ],
        out_specs=[pl.BlockSpec((own_depth * each, 128), lambda i: (0, 0)), row_block],
        out_shape=[
            jax.ShapeDtypeStruct((own_depth * each, 128), F32),
            jax.ShapeDtypeStruct((depth * each, 128), BF16),
        ],
        scratch_shapes=[
            pltpu.VMEM((span, width), BF16),
            pltpu.VMEM((maps, rank, cols), BF16),
            pltpu.VMEM((span * each, 128), F32),
        ],
        cost_estimate=pl.CostEstimate(
            flops=2 * depth * width * cols,
            transcendentals=0,
            bytes_accessed=2 * depth * width + 4 * depth * maps * cols,
        ),
        compiler_params=pltpu.CompilerParams(vmem_limit_bytes=40 << 20),
        name="low_rank_update",
    )(place, rate, own_factors, moments_mine, moments_other, *pieces, *weight_pieces)


def as_rows(array):
    depth, maps, cols = array.shape
    tiles = array.reshape(depth, maps, cols // 128, 128).transpose(0, 2, 1, 3)
    return tiles.reshape(depth * maps * cols // 128, 128)


def from_rows(rows, maps, cols):
    tiles = rows.reshape(-1, cols // 128, maps, 128).transpose(0, 2, 1, 3)
    return tiles.reshape(-1, maps, cols)


def sent_to_all(shard, axis):
    copies = jnp.broadcast_to(shard, (lax.axis_size(axis), *shard.shape))
    return lax.all_to_all(copies, axis, split_axis=0, concat_axis=0, tiled=True)


def turned(array, axis, distance):
    count = lax.axis_size(axis)
    return lax.ppermute(array, axis, [(i, (i + distance) % count) for i in range(count)])


def per_device(
    inputs, queries, keys, values, head_cot, mixing, head_gain, factors, moments, weights
):
    length = inputs.shape[0]
    planes = lax.axis_size(PLANE)
    fs_count = lax.axis_size(FS)
    groups = lax.axis_size("tp")
    token_factor = (length * fs_count) ** (-0.5)
    rank_here, maps, cols = moments.shape
    rank = rank_here * fs_count
    width = maps * rank
    place = jnp.stack([lax.axis_index(axis) for axis in (CORE, "tp", WIDE, DEEP)])
    own_factors = factors.reshape(-1, width)
    part = width // groups
    own_part = lax.dynamic_slice_in_dim(own_factors, lax.axis_index("tp") * part, part, 1)
    mine = sent_to_all(own_part, PLANE)
    weight_rows = lax.optimization_barrier(as_rows(weights)).astype(BF16)[None]
    weight_columns = [weight_rows] + [turned(weight_rows, DEEP, -n) for n in (4, 2, 6)]
    weight_columns = jnp.concatenate(weight_columns)
    d_query, d_value = attention_grads(queries, keys, values, head_cot, mixing, head_gain)
    mine, d_query, d_value, weight_columns = lax.optimization_barrier(
        (mine, d_query, d_value, weight_columns)
    )
    weight_columns = jnp.concatenate([weight_columns, turned(weight_columns, DEEP, -1)])
    other = turned(mine, CORE, 1)
    columns, reduced = reduce_inputs(place, mine, other, inputs)
    reduced, columns, weight_columns = lax.optimization_barrier(
        (sent_to_all(reduced, "tp"), columns, weight_columns)
    )
    pieces = [columns] + [turned(columns, "tp", n) for n in range(1, groups)]
    keep, send = project(token_factor, place, reduced, d_query, d_value)
    summed = (keep + turned(send, CORE, 1)).astype(BF16)
    summed = summed.reshape(planes, maps * rank_here, cols)
    summed, weight_columns = lax.optimization_barrier((summed, weight_columns))
    before = turned(weight_columns, WIDE, 1)
    after = turned(weight_columns, WIDE, -1)
    parts, before, after = lax.optimization_barrier(
        (lax.all_to_all(summed, PLANE, 0, 0, tiled=True), before, after)
    )
    projected = jnp.sum(parts.astype(F32), axis=0).reshape(maps, rank_here, cols)
    new_moments = BETA * moments + projected.transpose(1, 0, 2)
    sent = new_moments.astype(BF16).transpose(1, 0, 2).reshape(maps * rank_here, cols)
    half = before.shape[0] // 2
    across = [turned(before[:half], WIDE, 1), turned(after[half:], WIDE, -1)]
    moments_mine, pieces, across = lax.optimization_barrier(
        (sent_to_all(sent, PLANE), pieces, jnp.concatenate(across))
    )
    weight_pieces = [weight_columns, before, across, after]
    weight_pieces = [piece for mine in weight_pieces for piece in (mine, turned(mine, CORE, 1))]
    moments_other = turned(moments_mine, CORE, 1)
    squares = moments_mine.astype(F32) ** 2 + moments_other.astype(F32) ** 2
    squares = jnp.sum(squares.reshape(planes, maps, rank_here, cols), axis=(0, 2, 3))
    totals = squares
    for distance in range(1, groups):
        totals = totals + turned(squares, "tp", distance)
    rate = RATE_BASE / jnp.sqrt(1.0 + totals / (rank * cols * groups))
    step, copies = update(
        place,
        rate,
        own_factors,
        moments_mine.reshape(rank, cols),
        moments_other.reshape(rank, cols),
        pieces,
        weight_pieces,
    )
    return (from_rows(step, maps, cols), new_moments, from_rows(copies, maps, cols))


def solution(mesh):
    torus = Mesh(mesh.devices.reshape(8, 4, 2, mesh.shape["tp"]), (*FS, "tp"))
    placed = (
        P(FS, None),
        P(FS, "tp"),
        P(FS, "tp"),
        P(FS, "tp"),
        P(FS, "tp"),
        P("tp"),
        P(),
        P(FS, None, None),
        P(FS, None, "tp"),
        P(FS, None, "tp"),
    )
    return jax.shard_map(
        per_device,
        mesh=torus,
        in_specs=placed,
        out_specs=(P(FS, None, "tp"), P(FS, None, "tp"), P(None, None, "tp")),
        check_vma=False,
    )
```

```python
import functools

import jax
import jax.numpy as jnp
from jax import lax
from jax.experimental import pallas as pl
from jax.experimental.pallas import tpu as pltpu
from jax.sharding import Mesh
from jax.sharding import PartitionSpec as P

DEEP, WIDE, CORE = "fs_0", "fs_1", "fs_2"
PLANE = (DEEP, WIDE)
FS = (*PLANE, CORE)


EPS = 0.05
BETA = 0.9
RATE_BASE = 0.5
BF16 = jnp.bfloat16
F32 = jnp.float32


def nt_dot(left, right):
    return lax.dot_general(left, right, (((1,), (1,)), ((), ())), preferred_element_type=F32)


def tn_dot(left, right):
    return lax.dot_general(left, right, (((0,), (0,)), ((), ())), preferred_element_type=F32)


def attention_kernel(mix_ref, q_ref, k_ref, v_ref, up_ref, gain_ref, dq_ref, dv_ref):
    length = q_ref.shape[0]
    width = gain_ref.shape[1]
    heads = q_ref.shape[1] // width
    head_dim = width // 2
    factor = head_dim**-0.5
    gain = gain_ref[...]
    place = lax.broadcasted_iota(jnp.int32, (length, length), 0)
    causal = lax.broadcasted_iota(jnp.int32, (length, length), 1) <= place
    for head in range(heads):
        at = slice(head * width, (head + 1) * width)
        weight_mix = mix_ref[pl.program_id(0) * heads + head]
        query = q_ref[:, at]
        keys = k_ref[:, at]
        value = v_ref[:, at]

        def probs(which):
            cols = slice(which * head_dim, (which + 1) * head_dim)
            scores = nt_dot(query[:, cols], keys[:, cols]) * factor
            scores = jnp.where(causal, scores, -jnp.inf)
            expo = jnp.exp(scores - jnp.max(scores, axis=-1, keepdims=True))
            return expo * (1.0 / jnp.sum(expo, axis=-1, keepdims=True))

        first = probs(0)
        second = weight_mix * probs(1)
        mixed = (first - second).astype(BF16)
        output = jnp.dot(mixed, value, preferred_element_type=F32)
        inverse = lax.rsqrt(jnp.mean(output * output, axis=-1, keepdims=True) + EPS)
        scaled = gain * up_ref[:, at].astype(F32)
        along = jnp.mean(output * scaled, axis=-1, keepdims=True)
        d_out = (inverse * scaled - output * (inverse * inverse * inverse * along)).astype(BF16)
        dv_ref[:, at] = tn_dot(mixed, d_out).astype(BF16)
        d_mix = nt_dot(d_out, value)
        first_mix = jnp.sum(first * d_mix, axis=-1, keepdims=True)
        second_mix = jnp.sum(second * d_mix, axis=-1, keepdims=True) * (1.0 / weight_mix)
        d_first = (first * (d_mix - first_mix)).astype(BF16)
        d_second = (second * (second_mix - d_mix)).astype(BF16)
        dq_ref[:, head * width : head * width + head_dim] = (
            jnp.dot(d_first, keys[:, :head_dim], preferred_element_type=F32) * factor
        ).astype(BF16)
        dq_ref[:, head * width + head_dim : (head + 1) * width] = (
            jnp.dot(d_second, keys[:, head_dim:], preferred_element_type=F32) * factor
        ).astype(BF16)


def attention_grads(queries, keys, values, head_cot, mixing, head_gain, each=2):
    length, cols = queries.shape
    heads = mixing.shape[0]
    width = cols // heads
    block = pl.BlockSpec((length, each * width), lambda h: (0, h))
    return pl.pallas_call(
        attention_kernel,
        grid=(heads // each,),
        in_specs=[
            pl.BlockSpec(memory_space=pltpu.SMEM),
            block,
            block,
            block,
            block,
            pl.BlockSpec((1, width), lambda h: (0, 0)),
        ],
        out_specs=[block, block],
        out_shape=[jax.ShapeDtypeStruct((length, cols), BF16)] * 2,
        cost_estimate=pl.CostEstimate(
            flops=20 * length * length * cols,
            transcendentals=2 * heads * length * length,
            bytes_accessed=12 * length * cols,
        ),
        name="attention_grads",
    )(mixing, queries, keys, values, head_cot, head_gain.reshape(1, width))


def interleaved(first, second):
    half = lax.broadcasted_iota(jnp.int32, first.shape, 0) % 8 < 4
    count = first.shape[0]
    even = jnp.where(half, first, pltpu.roll(second, 4, 0))
    odd = jnp.where(half, pltpu.roll(first, count - 4, 0), second)
    return even, odd


def separated(even, odd):
    half = lax.broadcasted_iota(jnp.int32, even.shape, 0) % 8 < 4
    count = even.shape[0]
    first = jnp.where(half, even, pltpu.roll(odd, 4, 0))
    second = jnp.where(half, pltpu.roll(even, count - 4, 0), odd)
    return first, second


def reduce_kernel(core_ref, mine_ref, other_ref, in_ref, rows_ref, red_ref, sum_ref):
    step = pl.program_id(0)
    low = core_ref[0] == 0
    planes, rows, _ = mine_ref.shape
    for plane in range(planes):
        mine, other = mine_ref[plane], other_ref[plane]
        at = 2 * rows * plane
        rows_ref[at : at + rows, :] = jnp.where(low, mine, other)
        rows_ref[at + rows : at + 2 * rows, :] = jnp.where(low, other, mine)
    part = jnp.dot(in_ref[...], rows_ref[...], preferred_element_type=F32)

    @pl.when(step == 0)
    def _():
        sum_ref[...] = part

    @pl.when(step > 0)
    def _():
        sum_ref[...] += part

    @pl.when(step == pl.num_programs(0) - 1)
    def _():
        red_ref[...] = sum_ref[...].astype(BF16)


def reduce_inputs(core, mine, other, inputs, steps=2):
    planes, rows, width = mine.shape
    length, depth = inputs.shape
    block = pl.BlockSpec((planes // steps, rows, width), lambda i: (i, 0, 0))
    return pl.pallas_call(
        reduce_kernel,
        grid=(steps,),
        in_specs=[
            pl.BlockSpec(memory_space=pltpu.SMEM),
            block,
            block,
            pl.BlockSpec((length, depth // steps), lambda i: (0, i)),
        ],
        out_specs=[
            pl.BlockSpec((depth // steps, width), lambda i: (i, 0)),
            pl.BlockSpec((length, width), lambda i: (0, 0)),
        ],
        out_shape=[
            jax.ShapeDtypeStruct((depth, width), BF16),
            jax.ShapeDtypeStruct((length, width), BF16),
        ],
        scratch_shapes=[pltpu.VMEM((length, width), F32)],
        cost_estimate=pl.CostEstimate(
            flops=2 * length * width * depth,
            transcendentals=0,
            bytes_accessed=2 * depth * (length + 2 * width) + 2 * length * width,
        ),
        compiler_params=pltpu.CompilerParams(vmem_limit_bytes=32 << 20),
        name="reduce_inputs",
    )(core, mine, other, inputs)


def project_kernel(scale, core_ref, red_ref, dq_ref, dv_ref, keep_ref, send_ref):
    low = core_ref[0] == 0
    parts = red_ref.shape[0] // 2
    sums = []
    for k, cot_ref in enumerate((dq_ref, dv_ref)):
        reduced = jnp.concatenate([red_ref[k * parts + n] for n in range(parts)], axis=1)
        sums.append(tn_dot(reduced, cot_ref[...]) * scale)
    even, odd = interleaved(*sums)
    keep_ref[...] = jnp.where(low, even, odd)
    send_ref[...] = jnp.where(low, odd, even)


def project(scale, core, reduced, d_query, d_value):
    parts, length, width = reduced.shape
    cols = d_query.shape[1]
    rank = parts * width // 2
    whole = pl.BlockSpec((length, cols), lambda i: (0, 0))
    result = pl.BlockSpec((rank, cols), lambda i: (0, 0))
    return pl.pallas_call(
        functools.partial(project_kernel, scale),
        grid=(1,),
        in_specs=[
            pl.BlockSpec(memory_space=pltpu.SMEM),
            pl.BlockSpec((parts, length, width), lambda i: (0, 0, 0)),
            whole,
            whole,
        ],
        out_specs=[result, result],
        out_shape=[jax.ShapeDtypeStruct((rank, cols), F32)] * 2,
        cost_estimate=pl.CostEstimate(
            flops=4 * length * rank * cols,
            transcendentals=0,
            bytes_accessed=8 * length * cols + 8 * rank * cols,
        ),
        compiler_params=pltpu.CompilerParams(vmem_limit_bytes=32 << 20),
        name="project",
    )(core, reduced, d_query, d_value)


def low_rank_rows(scale_ref, factor_rows, moment_ref, rows_ref):
    maps, rank, cols = moment_ref.shape
    count = factor_rows.shape[0]
    tiles = cols // 128
    for k in range(maps):
        part = jnp.dot(
            factor_rows[:, k * rank : (k + 1) * rank], moment_ref[k], preferred_element_type=F32
        )
        part = part * scale_ref[k]
        for j in range(tiles):
            rows_ref[pl.ds(maps * j + k, count, stride=maps * tiles), :] = part[
                :, j * 128 : (j + 1) * 128
            ]


def update_kernel(groups, place_ref, scale_ref, own_ref, *refs):
    moment_mine_ref, moment_other_ref = refs[:2]
    piece_refs, weight_refs = refs[2 : 2 + groups], refs[2 + groups : -5]
    step_ref, copy_ref, factor_ref, moment_ref, rows_ref = refs[-5:]
    low = place_ref[0] == 0

    @pl.when(pl.program_id(0) == 0)
    def _():
        mine = moment_mine_ref[...].astype(F32)
        other = moment_other_ref[...].astype(F32)
        first, second = separated(jnp.where(low, mine, other), jnp.where(low, other, mine))
        moment_ref[0] = first.astype(BF16)
        moment_ref[1] = second.astype(BF16)
        low_rank_rows(scale_ref, own_ref[...], moment_ref, step_ref)

    for distance, piece_ref in enumerate(piece_refs):
        width = piece_ref.shape[1]
        at = lax.rem(place_ref[1] + (groups - distance), groups) * width
        factor_ref[:, pl.ds(pl.multiple_of(at, width), width)] = piece_ref[...]
    low_rank_rows(scale_ref, factor_ref[...], moment_ref, rows_ref)
    wide = len(weight_refs) // 2
    all_zs, count, _ = weight_refs[0].shape
    zs = copy_ref.shape[0] // (2 * wide * count)
    for distance in range(wide):
        mine_ref, other_ref = weight_refs[2 * distance : 2 * distance + 2]
        x = lax.rem(place_ref[2] + (wide - distance), wide)
        for z in range(zs):
            ahead = lax.rem(pl.program_id(0) * zs + z + all_zs - place_ref[3], all_zs)
            slot = 4 * lax.rem(ahead, 2) + 2 * lax.rem(ahead // 2, 2) + ahead // 4
            halves = mine_ref[slot], other_ref[slot]
            for owner in range(2):
                weight = jnp.where(low, halves[owner], halves[1 - owner])
                at = pl.multiple_of(count * (2 * (z * wide + x) + owner), count)
                part = pl.ds(at, count)
                copy_ref[part, :] = (weight.astype(F32) - rows_ref[part, :]).astype(BF16)


def update(place, rate, own_factors, moments_mine, moments_other, pieces, weight_pieces, steps=4):
    depth, part = pieces[0].shape
    own_depth, width = own_factors.shape
    rank, cols = moments_mine.shape
    maps = width // rank
    each = maps * cols // 128
    span = depth // steps
    moment_block = pl.BlockSpec((rank, cols), lambda i: (0, 0))
    row_block = pl.BlockSpec((span * each, 128), lambda i: (i, 0))
    weight_block = pl.BlockSpec(weight_pieces[0].shape, lambda i: (0, 0, 0))
    return pl.pallas_call(
        functools.partial(update_kernel, len(pieces)),
        grid=(steps,),
        in_specs=[
            pl.BlockSpec(memory_space=pltpu.SMEM),
            pl.BlockSpec(memory_space=pltpu.SMEM),
            pl.BlockSpec((own_depth, width), lambda i: (0, 0)),
            moment_block,
            moment_block,
            *[pl.BlockSpec((span, part), lambda i: (i, 0))] * len(pieces),
            *[weight_block] * len(weight_pieces),
        ],
        out_specs=[pl.BlockSpec((own_depth * each, 128), lambda i: (0, 0)), row_block],
        out_shape=[
            jax.ShapeDtypeStruct((own_depth * each, 128), F32),
            jax.ShapeDtypeStruct((depth * each, 128), BF16),
        ],
        scratch_shapes=[
            pltpu.VMEM((span, width), BF16),
            pltpu.VMEM((maps, rank, cols), BF16),
            pltpu.VMEM((span * each, 128), F32),
        ],
        cost_estimate=pl.CostEstimate(
            flops=2 * depth * width * cols,
            transcendentals=0,
            bytes_accessed=2 * depth * width + 4 * depth * maps * cols,
        ),
        compiler_params=pltpu.CompilerParams(vmem_limit_bytes=40 << 20),
        name="low_rank_update",
    )(place, rate, own_factors, moments_mine, moments_other, *pieces, *weight_pieces)


def as_rows(array):
    depth, maps, cols = array.shape
    tiles = array.reshape(depth, maps, cols // 128, 128).transpose(0, 2, 1, 3)
    return tiles.reshape(depth * maps * cols // 128, 128)


def from_rows(rows, maps, cols):
    tiles = rows.reshape(-1, cols // 128, maps, 128).transpose(0, 2, 1, 3)
    return tiles.reshape(-1, maps, cols)


def sent_to_all(shard, axis):
    copies = jnp.broadcast_to(shard, (lax.axis_size(axis), *shard.shape))
    return lax.all_to_all(copies, axis, split_axis=0, concat_axis=0, tiled=True)


def turned(array, axis, distance):
    count = lax.axis_size(axis)
    return lax.ppermute(array, axis, [(i, (i + distance) % count) for i in range(count)])


def per_device(
    inputs, queries, keys, values, head_cot, mixing, head_gain, factors, moments, weights
):
    length = inputs.shape[0]
    planes = lax.axis_size(PLANE)
    fs_count = lax.axis_size(FS)
    groups = lax.axis_size("tp")
    token_factor = (length * fs_count) ** (-0.5)
    rank_here, maps, cols = moments.shape
    rank = rank_here * fs_count
    width = maps * rank
    place = jnp.stack([lax.axis_index(axis) for axis in (CORE, "tp", WIDE, DEEP)])
    own_factors = factors.reshape(-1, width)
    part = width // groups
    own_part = lax.dynamic_slice_in_dim(own_factors, lax.axis_index("tp") * part, part, 1)
    mine = sent_to_all(own_part, PLANE)
    weight_rows = lax.optimization_barrier(as_rows(weights)).astype(BF16)[None]
    weight_columns = [weight_rows] + [turned(weight_rows, DEEP, -n) for n in (4, 2, 6)]
    weight_columns = jnp.concatenate(weight_columns)
    d_query, d_value = attention_grads(queries, keys, values, head_cot, mixing, head_gain)
    mine, d_query, d_value, weight_columns = lax.optimization_barrier(
        (mine, d_query, d_value, weight_columns)
    )
    weight_columns = jnp.concatenate([weight_columns, turned(weight_columns, DEEP, -1)])
    other = turned(mine, CORE, 1)
    columns, reduced = reduce_inputs(place, mine, other, inputs)
    reduced, columns, weight_columns = lax.optimization_barrier(
        (sent_to_all(reduced, "tp"), columns, weight_columns)
    )
    pieces = [columns] + [turned(columns, "tp", n) for n in range(1, groups)]
    keep, send = project(token_factor, place, reduced, d_query, d_value)
    summed = (keep + turned(send, CORE, 1)).astype(BF16)
    summed = summed.reshape(planes, maps * rank_here, cols)
    before = turned(weight_columns, WIDE, 1)
    after = turned(weight_columns, WIDE, -1)
    parts, before, after = lax.optimization_barrier(
        (lax.all_to_all(summed, PLANE, 0, 0, tiled=True), before, after)
    )
    projected = jnp.sum(parts.astype(F32), axis=0).reshape(maps, rank_here, cols)
    new_moments = BETA * moments + projected.transpose(1, 0, 2)
    sent = new_moments.astype(BF16).transpose(1, 0, 2).reshape(maps * rank_here, cols)
    half = before.shape[0] // 2
    across = [turned(before[:half], WIDE, 1), turned(after[half:], WIDE, -1)]
    moments_mine, pieces, across = lax.optimization_barrier(
        (sent_to_all(sent, PLANE), pieces, jnp.concatenate(across))
    )
    weight_pieces = [weight_columns, before, across, after]
    weight_pieces = [piece for mine in weight_pieces for piece in (mine, turned(mine, CORE, 1))]
    moments_other = turned(moments_mine, CORE, 1)
    squares = moments_mine.astype(F32) ** 2 + moments_other.astype(F32) ** 2
    squares = jnp.sum(squares.reshape(planes, maps, rank_here, cols), axis=(0, 2, 3))
    totals = squares
    for distance in range(1, groups):
        totals = totals + turned(squares, "tp", distance)
    rate = RATE_BASE / jnp.sqrt(1.0 + totals / (rank * cols * groups))
    step, copies = update(
        place,
        rate,
        own_factors,
        moments_mine.reshape(rank, cols),
        moments_other.reshape(rank, cols),
        pieces,
        weight_pieces,
    )
    return (from_rows(step, maps, cols), new_moments, from_rows(copies, maps, cols))


def solution(mesh):
    torus = Mesh(mesh.devices.reshape(8, 4, 2, mesh.shape["tp"]), (*FS, "tp"))
    placed = (
        P(FS, None),
        P(FS, "tp"),
        P(FS, "tp"),
        P(FS, "tp"),
        P(FS, "tp"),
        P("tp"),
        P(),
        P(FS, None, None),
        P(FS, None, "tp"),
        P(FS, None, "tp"),
    )
    return jax.shard_map(
        per_device,
        mesh=torus,
        in_specs=placed,
        out_specs=(P(FS, None, "tp"), P(FS, None, "tp"), P(None, None, "tp")),
        check_vma=False,
    )
```

```python
import functools

import jax
import jax.numpy as jnp
from jax import lax
from jax.experimental import pallas as pl
from jax.experimental.pallas import tpu as pltpu
from jax.sharding import Mesh
from jax.sharding import PartitionSpec as P

DEEP, WIDE, CORE = "fs_0", "fs_1", "fs_2"
PLANE = (DEEP, WIDE)
FS = (*PLANE, CORE)


EPS = 0.05
BETA = 0.9
RATE_BASE = 0.5
BF16 = jnp.bfloat16
F32 = jnp.float32


def nt_dot(left, right):
    return lax.dot_general(left, right, (((1,), (1,)), ((), ())), preferred_element_type=F32)


def tn_dot(left, right):
    return lax.dot_general(left, right, (((0,), (0,)), ((), ())), preferred_element_type=F32)


def attention_kernel(mix_ref, q_ref, k_ref, v_ref, up_ref, gain_ref, dq_ref, dv_ref):
    length = q_ref.shape[0]
    width = gain_ref.shape[1]
    heads = q_ref.shape[1] // width
    head_dim = width // 2
    factor = head_dim**-0.5
    gain = gain_ref[...]
    place = lax.broadcasted_iota(jnp.int32, (length, length), 0)
    causal = lax.broadcasted_iota(jnp.int32, (length, length), 1) <= place
    for head in range(heads):
        at = slice(head * width, (head + 1) * width)
        weight_mix = mix_ref[pl.program_id(0) * heads + head]
        query = q_ref[:, at]
        keys = k_ref[:, at]
        value = v_ref[:, at]

        def probs(which):
            cols = slice(which * head_dim, (which + 1) * head_dim)
            scores = nt_dot(query[:, cols], keys[:, cols]) * factor
            scores = jnp.where(causal, scores, -jnp.inf)
            expo = jnp.exp(scores - jnp.max(scores, axis=-1, keepdims=True))
            return expo * (1.0 / jnp.sum(expo, axis=-1, keepdims=True))

        first = probs(0)
        second = weight_mix * probs(1)
        mixed = (first - second).astype(BF16)
        output = jnp.dot(mixed, value, preferred_element_type=F32)
        inverse = lax.rsqrt(jnp.mean(output * output, axis=-1, keepdims=True) + EPS)
        scaled = gain * up_ref[:, at].astype(F32)
        along = jnp.mean(output * scaled, axis=-1, keepdims=True)
        d_out = (inverse * scaled - output * (inverse * inverse * inverse * along)).astype(BF16)
        dv_ref[:, at] = tn_dot(mixed, d_out).astype(BF16)
        d_mix = nt_dot(d_out, value)
        first_mix = jnp.sum(first * d_mix, axis=-1, keepdims=True)
        second_mix = jnp.sum(second * d_mix, axis=-1, keepdims=True) * (1.0 / weight_mix)
        d_first = (first * (d_mix - first_mix)).astype(BF16)
        d_second = (second * (second_mix - d_mix)).astype(BF16)
        dq_ref[:, head * width : head * width + head_dim] = (
            jnp.dot(d_first, keys[:, :head_dim], preferred_element_type=F32) * factor
        ).astype(BF16)
        dq_ref[:, head * width + head_dim : (head + 1) * width] = (
            jnp.dot(d_second, keys[:, head_dim:], preferred_element_type=F32) * factor
        ).astype(BF16)


def attention_grads(queries, keys, values, head_cot, mixing, head_gain, each=2):
    length, cols = queries.shape
    heads = mixing.shape[0]
    width = cols // heads
    block = pl.BlockSpec((length, each * width), lambda h: (0, h))
    return pl.pallas_call(
        attention_kernel,
        grid=(heads // each,),
        in_specs=[
            pl.BlockSpec(memory_space=pltpu.SMEM),
            block,
            block,
            block,
            block,
            pl.BlockSpec((1, width), lambda h: (0, 0)),
        ],
        out_specs=[block, block],
        out_shape=[jax.ShapeDtypeStruct((length, cols), BF16)] * 2,
        cost_estimate=pl.CostEstimate(
            flops=20 * length * length * cols,
            transcendentals=2 * heads * length * length,
            bytes_accessed=12 * length * cols,
        ),
        name="attention_grads",
    )(mixing, queries, keys, values, head_cot, head_gain.reshape(1, width))


def interleaved(first, second):
    half = lax.broadcasted_iota(jnp.int32, first.shape, 0) % 8 < 4
    count = first.shape[0]
    even = jnp.where(half, first, pltpu.roll(second, 4, 0))
    odd = jnp.where(half, pltpu.roll(first, count - 4, 0), second)
    return even, odd


def separated(even, odd):
    half = lax.broadcasted_iota(jnp.int32, even.shape, 0) % 8 < 4
    count = even.shape[0]
    first = jnp.where(half, even, pltpu.roll(odd, 4, 0))
    second = jnp.where(half, pltpu.roll(even, count - 4, 0), odd)
    return first, second


def reduce_kernel(core_ref, mine_ref, other_ref, in_ref, rows_ref, red_ref, sum_ref):
    step = pl.program_id(0)
    low = core_ref[0] == 0
    planes, rows, _ = mine_ref.shape
    for plane in range(planes):
        mine, other = mine_ref[plane], other_ref[plane]
        at = 2 * rows * plane
        rows_ref[at : at + rows, :] = jnp.where(low, mine, other)
        rows_ref[at + rows : at + 2 * rows, :] = jnp.where(low, other, mine)
    part = jnp.dot(in_ref[...], rows_ref[...], preferred_element_type=F32)

    @pl.when(step == 0)
    def _():
        sum_ref[...] = part

    @pl.when(step > 0)
    def _():
        sum_ref[...] += part

    @pl.when(step == pl.num_programs(0) - 1)
    def _():
        red_ref[...] = sum_ref[...].astype(BF16)


def reduce_inputs(core, mine, other, inputs, steps=2):
    planes, rows, width = mine.shape
    length, depth = inputs.shape
    block = pl.BlockSpec((planes // steps, rows, width), lambda i: (i, 0, 0))
    return pl.pallas_call(
        reduce_kernel,
        grid=(steps,),
        in_specs=[
            pl.BlockSpec(memory_space=pltpu.SMEM),
            block,
            block,
            pl.BlockSpec((length, depth // steps), lambda i: (0, i)),
        ],
        out_specs=[
            pl.BlockSpec((depth // steps, width), lambda i: (i, 0)),
            pl.BlockSpec((length, width), lambda i: (0, 0)),
        ],
        out_shape=[
            jax.ShapeDtypeStruct((depth, width), BF16),
            jax.ShapeDtypeStruct((length, width), BF16),
        ],
        scratch_shapes=[pltpu.VMEM((length, width), F32)],
        cost_estimate=pl.CostEstimate(
            flops=2 * length * width * depth,
            transcendentals=0,
            bytes_accessed=2 * depth * (length + 2 * width) + 2 * length * width,
        ),
        compiler_params=pltpu.CompilerParams(vmem_limit_bytes=32 << 20),
        name="reduce_inputs",
    )(core, mine, other, inputs)


def project_kernel(scale, core_ref, red_ref, dq_ref, dv_ref, keep_ref, send_ref):
    low = core_ref[0] == 0
    parts = red_ref.shape[0] // 2
    sums = []
    for k, cot_ref in enumerate((dq_ref, dv_ref)):
        reduced = jnp.concatenate([red_ref[k * parts + n] for n in range(parts)], axis=1)
        sums.append(tn_dot(reduced, cot_ref[...]) * scale)
    even, odd = interleaved(*sums)
    keep_ref[...] = jnp.where(low, even, odd)
    send_ref[...] = jnp.where(low, odd, even)


def project(scale, core, reduced, d_query, d_value):
    parts, length, width = reduced.shape
    cols = d_query.shape[1]
    rank = parts * width // 2
    whole = pl.BlockSpec((length, cols), lambda i: (0, 0))
    result = pl.BlockSpec((rank, cols), lambda i: (0, 0))
    return pl.pallas_call(
        functools.partial(project_kernel, scale),
        grid=(1,),
        in_specs=[
            pl.BlockSpec(memory_space=pltpu.SMEM),
            pl.BlockSpec((parts, length, width), lambda i: (0, 0, 0)),
            whole,
            whole,
        ],
        out_specs=[result, result],
        out_shape=[jax.ShapeDtypeStruct((rank, cols), F32)] * 2,
        cost_estimate=pl.CostEstimate(
            flops=4 * length * rank * cols,
            transcendentals=0,
            bytes_accessed=8 * length * cols + 8 * rank * cols,
        ),
        compiler_params=pltpu.CompilerParams(vmem_limit_bytes=32 << 20),
        name="project",
    )(core, reduced, d_query, d_value)


def low_rank_rows(scale_ref, factor_rows, moment_ref, rows_ref):
    maps, rank, cols = moment_ref.shape
    count = factor_rows.shape[0]
    tiles = cols // 128
    for k in range(maps):
        part = jnp.dot(
            factor_rows[:, k * rank : (k + 1) * rank], moment_ref[k], preferred_element_type=F32
        )
        part = part * scale_ref[k]
        for j in range(tiles):
            rows_ref[pl.ds(maps * j + k, count, stride=maps * tiles), :] = part[
                :, j * 128 : (j + 1) * 128
            ]


def update_kernel(groups, place_ref, scale_ref, own_ref, *refs):
    moment_mine_ref, moment_other_ref = refs[:2]
    piece_refs, weight_refs = refs[2 : 2 + groups], refs[2 + groups : -5]
    step_ref, copy_ref, factor_ref, moment_ref, rows_ref = refs[-5:]
    low = place_ref[0] == 0

    @pl.when(pl.program_id(0) == 0)
    def _():
        mine = moment_mine_ref[...].astype(F32)
        other = moment_other_ref[...].astype(F32)
        first, second = separated(jnp.where(low, mine, other), jnp.where(low, other, mine))
        moment_ref[0] = first.astype(BF16)
        moment_ref[1] = second.astype(BF16)
        low_rank_rows(scale_ref, own_ref[...], moment_ref, step_ref)

    for distance, piece_ref in enumerate(piece_refs):
        width = piece_ref.shape[1]
        at = lax.rem(place_ref[1] + (groups - distance), groups) * width
        factor_ref[:, pl.ds(pl.multiple_of(at, width), width)] = piece_ref[...]
    low_rank_rows(scale_ref, factor_ref[...], moment_ref, rows_ref)
    wide = len(weight_refs) // 2
    all_zs, count, _ = weight_refs[0].shape
    zs = copy_ref.shape[0] // (2 * wide * count)
    for distance in range(wide):
        mine_ref, other_ref = weight_refs[2 * distance : 2 * distance + 2]
        x = lax.rem(place_ref[2] + (wide - distance), wide)
        for z in range(zs):
            ahead = lax.rem(pl.program_id(0) * zs + z + all_zs - place_ref[3], all_zs)
            slot = 4 * lax.rem(ahead, 2) + 2 * lax.rem(ahead // 2, 2) + ahead // 4
            halves = mine_ref[slot], other_ref[slot]
            for owner in range(2):
                weight = jnp.where(low, halves[owner], halves[1 - owner])
                at = pl.multiple_of(count * (2 * (z * wide + x) + owner), count)
                part = pl.ds(at, count)
                copy_ref[part, :] = (weight.astype(F32) - rows_ref[part, :]).astype(BF16)


def update(place, rate, own_factors, moments_mine, moments_other, pieces, weight_pieces, steps=4):
    depth, part = pieces[0].shape
    own_depth, width = own_factors.shape
    rank, cols = moments_mine.shape
    maps = width // rank
    each = maps * cols // 128
    span = depth // steps
    moment_block = pl.BlockSpec((rank, cols), lambda i: (0, 0))
    row_block = pl.BlockSpec((span * each, 128), lambda i: (i, 0))
    weight_block = pl.BlockSpec(weight_pieces[0].shape, lambda i: (0, 0, 0))
    return pl.pallas_call(
        functools.partial(update_kernel, len(pieces)),
        grid=(steps,),
        in_specs=[
            pl.BlockSpec(memory_space=pltpu.SMEM),
            pl.BlockSpec(memory_space=pltpu.SMEM),
            pl.BlockSpec((own_depth, width), lambda i: (0, 0)),
            moment_block,
            moment_block,
            *[pl.BlockSpec((span, part), lambda i: (i, 0))] * len(pieces),
            *[weight_block] * len(weight_pieces),
        ],
        out_specs=[pl.BlockSpec((own_depth * each, 128), lambda i: (0, 0)), row_block],
        out_shape=[
            jax.ShapeDtypeStruct((own_depth * each, 128), F32),
            jax.ShapeDtypeStruct((depth * each, 128), BF16),
        ],
        scratch_shapes=[
            pltpu.VMEM((span, width), BF16),
            pltpu.VMEM((maps, rank, cols), BF16),
            pltpu.VMEM((span * each, 128), F32),
        ],
        cost_estimate=pl.CostEstimate(
            flops=2 * depth * width * cols,
            transcendentals=0,
            bytes_accessed=2 * depth * width + 4 * depth * maps * cols,
        ),
        compiler_params=pltpu.CompilerParams(vmem_limit_bytes=40 << 20),
        name="low_rank_update",
    )(place, rate, own_factors, moments_mine, moments_other, *pieces, *weight_pieces)


def as_rows(array):
    depth, maps, cols = array.shape
    tiles = array.reshape(depth, maps, cols // 128, 128).transpose(0, 2, 1, 3)
    return tiles.reshape(depth * maps * cols // 128, 128)


def from_rows(rows, maps, cols):
    tiles = rows.reshape(-1, cols // 128, maps, 128).transpose(0, 2, 1, 3)
    return tiles.reshape(-1, maps, cols)


def sent_to_all(shard, axis):
    copies = jnp.broadcast_to(shard, (lax.axis_size(axis), *shard.shape))
    return lax.all_to_all(copies, axis, split_axis=0, concat_axis=0, tiled=True)


def turned(array, axis, distance):
    count = lax.axis_size(axis)
    return lax.ppermute(array, axis, [(i, (i + distance) % count) for i in range(count)])


def per_device(
    inputs, queries, keys, values, head_cot, mixing, head_gain, factors, moments, weights
):
    length = inputs.shape[0]
    planes = lax.axis_size(PLANE)
    fs_count = lax.axis_size(FS)
    groups = lax.axis_size("tp")
    token_factor = (length * fs_count) ** (-0.5)
    rank_here, maps, cols = moments.shape
    rank = rank_here * fs_count
    width = maps * rank
    place = jnp.stack([lax.axis_index(axis) for axis in (CORE, "tp", WIDE, DEEP)])
    own_factors = factors.reshape(-1, width)
    part = width // groups
    own_part = lax.dynamic_slice_in_dim(own_factors, lax.axis_index("tp") * part, part, 1)
    weight_rows = lax.optimization_barrier(as_rows(weights)).astype(BF16)[None]
    ahead = [turned(weight_rows, DEEP, -n) for n in (4, 2)]
    mine = sent_to_all(own_part, PLANE)
    ahead.append(turned(weight_rows, DEEP, -6))
    weight_columns = jnp.concatenate([weight_rows, *ahead])
    d_query, d_value = attention_grads(queries, keys, values, head_cot, mixing, head_gain)
    mine, d_query, d_value, weight_columns = lax.optimization_barrier(
        (mine, d_query, d_value, weight_columns)
    )
    weight_columns = jnp.concatenate([weight_columns, turned(weight_columns, DEEP, -1)])
    other = turned(mine, CORE, 1)
    columns, reduced = reduce_inputs(place, mine, other, inputs)
    reduced, columns, weight_columns = lax.optimization_barrier(
        (sent_to_all(reduced, "tp"), columns, weight_columns)
    )
    pieces = [columns] + [turned(columns, "tp", n) for n in range(1, groups)]
    keep, send = project(token_factor, place, reduced, d_query, d_value)
    summed = (keep + turned(send, CORE, 1)).astype(BF16)
    summed = summed.reshape(planes, maps * rank_here, cols)
    before = turned(weight_columns, WIDE, 1)
    after = turned(weight_columns, WIDE, -1)
    parts, before, after = lax.optimization_barrier(
        (lax.all_to_all(summed, PLANE, 0, 0, tiled=True), before, after)
    )
    projected = jnp.sum(parts.astype(F32), axis=0).reshape(maps, rank_here, cols)
    new_moments = BETA * moments + projected.transpose(1, 0, 2)
    sent = new_moments.astype(BF16).transpose(1, 0, 2).reshape(maps * rank_here, cols)
    half = before.shape[0] // 2
    across = [turned(before[:half], WIDE, 1), turned(after[half:], WIDE, -1)]
    moments_mine, pieces, across = lax.optimization_barrier(
        (sent_to_all(sent, PLANE), pieces, jnp.concatenate(across))
    )
    weight_pieces = [weight_columns, before, across, after]
    weight_pieces = [piece for mine in weight_pieces for piece in (mine, turned(mine, CORE, 1))]
    moments_other = turned(moments_mine, CORE, 1)
    squares = moments_mine.astype(F32) ** 2 + moments_other.astype(F32) ** 2
    squares = jnp.sum(squares.reshape(planes, maps, rank_here, cols), axis=(0, 2, 3))
    totals = squares
    for distance in range(1, groups):
        totals = totals + turned(squares, "tp", distance)
    rate = RATE_BASE / jnp.sqrt(1.0 + totals / (rank * cols * groups))
    step, copies = update(
        place,
        rate,
        own_factors,
        moments_mine.reshape(rank, cols),
        moments_other.reshape(rank, cols),
        pieces,
        weight_pieces,
    )
    return (from_rows(step, maps, cols), new_moments, from_rows(copies, maps, cols))


def solution(mesh):
    torus = Mesh(mesh.devices.reshape(8, 4, 2, mesh.shape["tp"]), (*FS, "tp"))
    placed = (
        P(FS, None),
        P(FS, "tp"),
        P(FS, "tp"),
        P(FS, "tp"),
        P(FS, "tp"),
        P("tp"),
        P(),
        P(FS, None, None),
        P(FS, None, "tp"),
        P(FS, None, "tp"),
    )
    return jax.shard_map(
        per_device,
        mesh=torus,
        in_specs=placed,
        out_specs=(P(FS, None, "tp"), P(FS, None, "tp"), P(None, None, "tp")),
        check_vma=False,
    )
```
